128 devices in a mesh: sp: 16 (over z, y), tp: 8 (over x, core).
Axes of the slice: x: 4, y: 4, z: 4, core: 2. Of those that a mesh axis runs over, the one named last changes fastest.
Arguments:
- resid: bfloat16 [16384, 2048], P(('sp', 'tp')), may hold values from -6 to 6
- query_nope: bfloat16 [16384, 2048], P('sp', 'tp'), may hold values from -18 to 18
- query_rope: bfloat16 [16384, 1024], P('sp', 'tp'), may hold values from -300 to 300
- latent: bfloat16 [16384, 256], P('sp'), may hold values from -6 to 6
- key_rope: bfloat16 [16384, 64], P('sp'), may hold values from -6 to 6
- latent_gain: float32 [256], replicated, may hold values from 0.1 to 1.9
- w_key: bfloat16 [256, 2048], P(None, 'tp'), may hold values from -0.375 to 0.375
- w_value: bfloat16 [256, 2048], P(None, 'tp'), may hold values from -0.375 to 0.375
- w_out: bfloat16 [2048, 2048], P('tp'), may hold values from -0.125 to 0.125
- mix_gain: float32 [2048], replicated, may hold values from 0.1 to 1.9
- w_gate: bfloat16 [2048, 5632], P('sp', 'tp'), may hold values from -0.125 to 0.125
- w_up: bfloat16 [2048, 5632], P('sp', 'tp'), may hold values from -0.125 to 0.125
- w_down: bfloat16 [2048, 5632], P('sp', 'tp'), may hold values from -0.078125 to 0.078125
Outputs:
- layer_out: bfloat16 [16384, 2048], P(('sp', 'tp'))
The draws below stay inside these ranges and needn't reach their ends.
All inputs are finite; a program needn't handle non-finite values.
Results may differ from the reference program's by a relative error of at most 0.0095.
Values may be sent and summed in bfloat16 or wider, within the bound.
A program may use at most 128 MiB of HBM per device.

```python
import jax
import jax.numpy as jnp
from jax import lax

D = 2048
HEADS = 16
NOPE = 128
ROPE = 64
VDIM = 128
RANK = 256
FF = 5632
TOK_DEV = 1024
TOKENS = 16384
N_SP = 16
N_TP = 8


def rope_pair(key):
    base_key = jax.random.fold_in(key, 11)
    key_one, key_two = jax.random.split(base_key, 2)
    key_part = jax.random.truncated_normal(key_one, -5.0, 5.0, (TOKENS, ROPE), jnp.float32)
    query_part = 3.0 * jax.random.truncated_normal(key_two, -5.0, 5.0, (TOKENS, HEADS * ROPE), jnp.float32)
    return (key_part, query_part)


def draw_query_rope(key, part):
    return rope_pair(key)[1].astype(jnp.bfloat16)


def draw_key_rope(key, part):
    return rope_pair(key)[0].astype(jnp.bfloat16)


def block_levels(key, dims, cuts, least, top_value):
    def one(position, blocks):
        heights = jax.random.uniform(jax.random.fold_in(jax.random.fold_in(key, 6), position), (blocks,), jnp.float32, least / len(cuts), top_value / len(cuts))
        return jnp.repeat(jnp.exp(heights), dims[position] // blocks).reshape((-1,) + (1,) * (len(dims) - position - 1))

    factor_of = one(*cuts[0])
    for cut in cuts[1:]:
        factor_of = factor_of * one(*cut)
    return factor_of


def bell_draw(stream_key, dims, spread, reach, cuts=(), held_as=jnp.bfloat16):
    loudness = block_levels(stream_key, dims, cuts, -0.22, 0.18) if cuts else 1.0
    result = jax.random.normal(stream_key, dims, jnp.float32) * spread * loudness
    return jnp.minimum(jnp.maximum(result, -reach), reach).astype(held_as)


def setup_inputs(seed: int = 0) -> dict:
    splits = jax.random.split(jax.random.key(seed), 14)
    resid = bell_draw(splits[0], (TOKENS, D), 1.0, 6.0, ((0, 128),))
    query_nope = bell_draw(splits[1], (TOKENS, HEADS * NOPE), 3.0, 18.0, ((0, 16), (1, 8)))
    query_rope = draw_query_rope(jax.random.fold_in(splits[13], 71), 0)
    latent = bell_draw(splits[3], (TOKENS, RANK), 1.0, 6.0, ((0, 16),))
    key_rope = draw_key_rope(jax.random.fold_in(splits[13], 71), 0)
    latent_gain = jnp.clip(1.0 + 0.18 * jax.random.normal(splits[5], (RANK,), jnp.float32), 0.1, 1.9)
    w_key = bell_draw(splits[6], (RANK, HEADS * NOPE), RANK ** -0.5, 0.375, ((1, 8),))
    w_value = bell_draw(splits[7], (RANK, HEADS * VDIM), RANK ** -0.5, 0.375, ((1, 8),))
    w_out = bell_draw(splits[8], (HEADS * VDIM, D), (HEADS * VDIM) ** -0.5, 0.125, ((0, 8),))
    mix_gain = jnp.clip(1.0 + 0.18 * jax.random.normal(splits[9], (D,), jnp.float32), 0.1, 1.9)
    w_gate = bell_draw(splits[10], (D, FF), D ** -0.5, 0.125, ((0, 16), (1, 8)))
    w_up = bell_draw(splits[11], (D, FF), D ** -0.5, 0.125, ((0, 16), (1, 8)))
    w_down = bell_draw(splits[12], (D, FF), FF ** -0.5, 0.078125, ((0, 16), (1, 8)))
    return {"resid": resid, "query_nope": query_nope, "query_rope": query_rope, "latent": latent, "key_rope": key_rope, "latent_gain": latent_gain, "w_key": w_key, "w_value": w_value, "w_out": w_out, "mix_gain": mix_gain, "w_gate": w_gate, "w_up": w_up, "w_down": w_down}


norm_eps = 1e-06
masked_score = -1e+30
theta_base = 10000.0

def rotate(values_in, angle):
    half_width = values_in.shape[-1] // 2
    front_half = values_in[..., :half_width]
    back_half = values_in[..., half_width:]
    cosine = jnp.cos(angle)
    sine_part = jnp.sin(angle)
    return jnp.concatenate([front_half * cosine - back_half * sine_part, back_half * cosine + front_half * sine_part], axis=-1)

def angles(positions, full_width):
    half_width = full_width // 2
    frequency = theta_base ** (-2.0 * jnp.arange(half_width).astype(jnp.float32) / full_width)
    return positions[:, None] * frequency[None, :]

def rms_scale(values_in, gain):
    return values_in * lax.rsqrt(lax.optimization_barrier(jnp.mean(values_in * values_in, axis=-1, keepdims=True)) + norm_eps) * gain

def reference(resid, query_nope, query_rope, latent, key_rope, latent_gain, w_key, w_value, w_out, mix_gain, w_gate, w_up, w_down):
    positions = jnp.arange(TOKENS).astype(jnp.float32)
    angle = angles(positions, ROPE)
    latent_normed = rms_scale(latent.astype(jnp.float32), latent_gain).astype(jnp.bfloat16)
    head_keys = jnp.dot(latent_normed, w_key, preferred_element_type=jnp.float32).astype(jnp.bfloat16)
    head_values = jnp.dot(latent_normed, w_value, preferred_element_type=jnp.float32).astype(jnp.bfloat16)
    key_rotated = rotate(key_rope.astype(jnp.float32), angle).astype(jnp.bfloat16)
    query_rotated = rotate(query_rope.astype(jnp.float32).reshape(TOKENS, HEADS, ROPE), angle[:, None, :]).astype(jnp.bfloat16)
    by_head_nope = jnp.transpose(query_nope.reshape(TOKENS, HEADS, NOPE), (1, 0, 2))
    by_head_rope = jnp.transpose(query_rotated, (1, 0, 2))
    by_head_keys = jnp.transpose(head_keys.reshape(TOKENS, HEADS, NOPE), (1, 0, 2))
    by_head_values = jnp.transpose(head_values.reshape(TOKENS, HEADS, VDIM), (1, 0, 2))
    score_scale = (NOPE + ROPE) ** (-0.5)
    key_positions = jnp.arange(TOKENS).astype(jnp.int32)

    def one_head(operands):
        nope_q, rope_q, keys_h, values_h = operands

        def one_block(block_index):
            first_row = block_index * TOK_DEV
            query_part = lax.dynamic_slice_in_dim(nope_q, first_row, TOK_DEV, 0)
            rope_part = lax.dynamic_slice_in_dim(rope_q, first_row, TOK_DEV, 0)
            scores = jnp.dot(query_part, keys_h.T, preferred_element_type=jnp.float32)
            scores = (scores + jnp.dot(rope_part, key_rotated.T, preferred_element_type=jnp.float32)) * score_scale
            query_rows = first_row + jnp.arange(TOK_DEV).astype(jnp.int32)
            causal = key_positions[None, :] <= query_rows[:, None]
            scores = jnp.where(causal, scores, masked_score)
            row_max = lax.optimization_barrier(jnp.max(scores, axis=-1, keepdims=True))
            weights = jnp.where(causal, jnp.exp(scores - row_max), 0.0)
            weight_sum = lax.optimization_barrier(jnp.sum(weights, axis=-1, keepdims=True))
            mixed = jnp.dot(weights.astype(jnp.bfloat16), values_h, preferred_element_type=jnp.float32)
            return (mixed / weight_sum).astype(jnp.bfloat16)
        return lax.map(one_block, jnp.arange(N_SP).astype(jnp.int32))
    head_out = lax.map(one_head, (by_head_nope, by_head_rope, by_head_keys, by_head_values))
    head_out = head_out.reshape(HEADS, TOKENS, VDIM)
    group_heads = HEADS // N_TP
    out_heads = w_out.reshape(HEADS, VDIM, D)
    attention_proj = jnp.zeros((TOKENS, D), jnp.float32)
    for group_index in range(N_TP):
        picked = slice(group_index * group_heads, (group_index + 1) * group_heads)
        partial_sum = jnp.einsum('htv,hvd->td', head_out[picked].astype(jnp.float32), out_heads[picked].astype(jnp.float32))
        attention_proj = attention_proj + lax.optimization_barrier(partial_sum.astype(jnp.bfloat16)).astype(jnp.float32)
    stream = resid.astype(jnp.float32) + attention_proj
    normed = rms_scale(stream, mix_gain).astype(jnp.bfloat16)
    group_units = FF // N_TP
    mixer_out = jnp.zeros((TOKENS, D), jnp.float32)
    for group_index in range(N_TP):
        columns = slice(group_index * group_units, (group_index + 1) * group_units)
        gate_value = jnp.dot(normed, w_gate[:, columns], preferred_element_type=jnp.float32)
        upward = jnp.dot(normed, w_up[:, columns], preferred_element_type=jnp.float32)
        hidden = (jax.nn.silu(gate_value) * upward).astype(jnp.bfloat16)
        partial_sum = jnp.dot(hidden, w_down[:, columns].T, preferred_element_type=jnp.float32)
        mixer_out = mixer_out + lax.optimization_barrier(partial_sum.astype(jnp.bfloat16)).astype(jnp.float32)
    return (stream + 0.5 * mixer_out).astype(jnp.bfloat16)
```

```python
import functools

import jax
import jax.numpy as jnp
from jax import lax
from jax.experimental import pallas as pl
from jax.experimental.pallas import tpu as pltpu
from jax.sharding import PartitionSpec as P

NOPE = 128
ROPE = 64
VDIM = 128
ROWS = 1024
HALF = 512
SIDE = 4
SHARD = HALF + HALF // 4

norm_eps = 1e-06
masked_score = -1e30
theta_base = 10000.0
score_base2 = (NOPE + ROPE) ** (-0.5) * 1.4426950408889634
MESH = pl.DeviceIdType.MESH

ORDER = ((0, 0), (1, 0), (3, 0), (0, 1), (0, 3), (2, 0), (0, 2), (1, 1), (1, 3), (3, 1), (3, 3),
         (2, 1), (2, 3), (1, 2), (3, 2), (2, 2))
PLACE = {pair: p for p, pair in enumerate(ORDER)}
ALPHA, BETA, FULL = (0, 320), (320, 320), (0, 640)
ALPHA0, ALPHA1, BETA0, BETA1 = (0, 160), (160, 160), (320, 160), (480, 160)

SENDS = (
    (((0, 0), FULL, (1, 0), 0), ((0, 0), FULL, (-1, 0), 0), ((0, 0), FULL, (0, 1), 0), ((0, 0), FULL, (0, -1), 0)),
    (
        ((1, 0), ALPHA, (-1, 0), 0), ((3, 0), BETA, (1, 0), 1),
        ((0, 1), ALPHA, (0, -1), 0), ((0, 3), BETA, (0, 1), 1),
        ((1, 0), ALPHA, (0, 1), 0), ((1, 0), ALPHA, (0, -1), 0),
        ((3, 0), ALPHA, (0, 1), 0), ((3, 0), ALPHA, (0, -1), 0),
        ((0, 1), BETA, (1, 0), 1), ((0, 1), BETA, (-1, 0), 1),
        ((0, 3), BETA, (1, 0), 1), ((0, 3), BETA, (-1, 0), 1),
    ),
    (
        ((2, 0), ALPHA, (0, 1), 0), ((2, 0), ALPHA, (0, -1), 0),
        ((0, 2), BETA, (1, 0), 1), ((0, 2), BETA, (-1, 0), 1),
    ),
    (
        ((1, 1), ALPHA0, (0, -1), 0), ((1, 3), ALPHA1, (0, 1), 2),
        ((3, 1), ALPHA0, (0, -1), 0), ((3, 3), ALPHA1, (0, 1), 2),
        ((1, 1), BETA0, (-1, 0), 1), ((3, 1), BETA1, (1, 0), 2),
        ((1, 3), BETA0, (-1, 0), 1), ((3, 3), BETA1, (1, 0), 2),
    ),
    (
        ((2, 1), ALPHA0, (0, -1), 0), ((2, 3), ALPHA1, (0, 1), 1),
        ((1, 2), BETA0, (-1, 0), 2), ((3, 2), BETA1, (1, 0), 3),
    ),
)


def at_receiver(source, step):
    return PLACE[((source[0] - step[0]) % SIDE, (source[1] - step[1]) % SIDE)]


def pick(index, values):
    found = jnp.int32(values[0])
    for at in range(1, len(values)):
        found = jnp.where(index == at, jnp.int32(values[at]), found)
    return found


def attention_kernel(
    nope, rope, shard, w_key, w_value, w_out, heads_all, w_out_all,
    lat, far_nope, far_rope, queries, keys, values_t, w_value_t, top, total, acc, head_out,
    send_sem, recv_sem, pair_send, pair_recv, query_send, query_recv, head_send, head_recv,
    out_send, out_recv, local_sem,
):
    s = lax.axis_index("sp")
    t = lax.axis_index("tp")
    z, y = s // SIDE, s % SIDE
    x, core = t // 2, t % 2
    mirror = 15 - s

    def sp_at(dy, dz):
        return ((z + dz + SIDE) % SIDE) * SIDE + (y + dy + SIDE) % SIDE

    def tp_at(dx):
        return ((x + dx + SIDE) % SIDE) * 2 + core

    partner = x * 2 + 1 - core

    barrier = pltpu.get_barrier_semaphore()
    for step in (1, 2, 3):
        pl.semaphore_signal(barrier, inc=1, device_id=(sp_at(step, 0), t), device_id_type=MESH)
        pl.semaphore_signal(barrier, inc=1, device_id=(sp_at(0, step), t), device_id_type=MESH)
    for step in range(1, 8):
        pl.semaphore_signal(barrier, inc=1, device_id=(s, (t + step) % 8), device_id_type=MESH)
    for step in range(8):
        pl.semaphore_signal(barrier, inc=1, device_id=(mirror, (t + step) % 8), device_id_type=MESH)
    pl.semaphore_wait(barrier, 21)

    def query_copies():
        return (
            pltpu.make_async_remote_copy(
                nope.at[pl.ds(HALF, HALF)], far_nope, query_send.at[0], query_recv.at[0],
                device_id=(mirror, t), device_id_type=MESH),
            pltpu.make_async_remote_copy(
                rope.at[pl.ds(HALF, HALF)], far_rope, query_send.at[1], query_recv.at[1],
                device_id=(mirror, t), device_id_type=MESH),
        )

    for copy in query_copies():
        copy.start()

    own = 2 * s + core

    def relative(pair, plane):
        return 2 * sp_at(*pair) + plane

    def shard_copy(phase, index):
        source, (first, count), step, slot = SENDS[phase][index]
        number = sum(len(one) for one in SENDS[:phase]) + index
        place = at_receiver(source, step)
        block = relative(source, core)
        if phase == 0:
            source_ref = shard
        else:
            source_ref = lat.at[block, pl.ds(first, count)]
        return pltpu.make_async_remote_copy(
            source_ref, lat.at[block, pl.ds(first, count)],
            send_sem.at[number], recv_sem.at[4 * place + slot],
            device_id=(sp_at(*step), t), device_id_type=MESH)

    def start_phase(phase):
        for index in range(len(SENDS[phase])):
            shard_copy(phase, index).start()

    def wait_received(phase):
        for index, (source, (first, count), step, slot) in enumerate(SENDS[phase]):
            place = at_receiver(source, step)
            block = relative(ORDER[place], core)
            pltpu.make_async_remote_copy(
                lat.at[block, pl.ds(first, count)], lat.at[block, pl.ds(first, count)],
                send_sem.at[0], recv_sem.at[4 * place + slot],
                device_id=(sp_at(*step), t), device_id_type=MESH).wait_recv()

    def pair_copy(place):
        block = relative(ORDER[place], core)
        return pltpu.make_async_remote_copy(
            shard if place == 0 else lat.at[block], lat.at[block],
            pair_send.at[place], pair_recv.at[place],
            device_id=(s, partner), device_id_type=MESH)

    def out_copy(number, slot, rows, target):
        first, count = rows
        source = w_out.at[pl.ds(first, count)] if number < 3 else w_out_all.at[slot, pl.ds(first, count)]
        return pltpu.make_async_remote_copy(
            source, w_out_all.at[slot, pl.ds(first, count)],
            out_send.at[number], out_recv.at[number],
            device_id=(s, target), device_id_type=MESH)

    whole, upper, lower = (0, 256), (0, 128), (128, 128)
    right, left, across = tp_at(1), tp_at(3), tp_at(2)
    out_sends = (
        (0, t, whole, right), (1, t, whole, left), (2, t, whole, partner),
        (3, right, upper, left), (4, left, lower, right),
        (5, right, whole, partner), (6, left, whole, partner), (7, across, whole, partner),
    )

    def other(slot):
        return (slot // 2) * 2 + 1 - slot % 2

    out_receives = (
        (0, left, whole), (1, right, whole), (2, partner, whole),
        (3, across, upper), (4, across, lower),
        (5, other(right), whole), (6, other(left), whole), (7, other(across), whole),
    )

    def out_wait(number):
        _, slot, (first, count) = out_receives[number]
        pltpu.make_async_remote_copy(
            w_out_all.at[slot, pl.ds(first, count)], w_out_all.at[slot, pl.ds(first, count)],
            out_send.at[number], out_recv.at[number],
            device_id=(s, partner), device_id_type=MESH).wait_recv()

    start_phase(0)
    pair_copy(0).start()
    for number in range(3):
        out_copy(*out_sends[number]).start()
    own_shard = pltpu.make_async_copy(shard, lat.at[own], local_sem.at[0])
    own_shard.start()
    own_out = pltpu.make_async_copy(w_out, w_out_all.at[t], local_sem.at[1])
    own_out.start()

    w_value_t[...] = jnp.transpose(w_value[...].astype(jnp.float32)).astype(jnp.bfloat16)
    top[...] = jnp.full_like(top, masked_score)
    total[...] = jnp.zeros_like(total)
    acc[...] = jnp.zeros_like(acc)

    lanes = lax.broadcasted_iota(jnp.int32, (HALF, 128), 1)

    def set_queries(group, nope_rows, rope_rows):
        wide = rope_rows.astype(jnp.float32)
        turned = pltpu.roll(wide, 64, 1)
        front = lanes < 64
        for head in range(2):
            one = nope_rows[:, head * NOPE:(head + 1) * NOPE]
            low, high = (wide, turned) if head == 0 else (turned, wide)
            for version, tail in enumerate((jnp.where(front, low, 0.0), jnp.where(front, 0.0, high))):
                queries[group, head, version, :, 0:NOPE] = one
                queries[group, head, version, :, NOPE:2 * NOPE] = tail.astype(jnp.bfloat16)

    set_queries(0, nope[pl.ds(0, HALF), :], rope[pl.ds(0, HALF), :])
    own_shard.wait()
    for copy in query_copies():
        copy.wait_recv()
    set_queries(1, far_nope[...], far_rope[...])

    last_near, last_far = 2 * s, 31 - 2 * s

    def expand(block):
        rows = lat[block, pl.ds(0, HALF), :]
        expanded = jnp.dot(rows, w_key[...], preferred_element_type=jnp.float32).astype(jnp.bfloat16)
        tails = (lat[block, pl.ds(HALF, 128), 0:128], lat[block, pl.ds(HALF, 128), 128:256])
        for head in range(2):
            keys[head, :, 0:NOPE] = expanded[:, head * NOPE:(head + 1) * NOPE]
            for quarter in range(4):
                keys[head, pl.ds(quarter * 128, 128), NOPE:2 * NOPE] = tails[quarter % 2]
        values_t[...] = lax.dot_general(
            w_value_t[...], rows, (((1,), (1,)), ((), ())), preferred_element_type=jnp.float32
        ).astype(jnp.bfloat16)

    def fold(group, masked):
        for head in range(2):
            scores = jnp.concatenate(
                [
                    lax.dot_general(
                        keys[head, pl.ds(256 * version, 256), :], queries[group, head, version],
                        (((1,), (1,)), ((), ())), preferred_element_type=jnp.float32)
                    for version in range(2)
                ],
                axis=0,
            )
            if masked:
                key_at = lax.broadcasted_iota(jnp.int32, scores.shape, 0)
                query_at = lax.broadcasted_iota(jnp.int32, scores.shape, 1)
                scores = jnp.where(key_at <= query_at, scores, masked_score)
            before = top[group, head]
            after = jnp.maximum(before, jnp.max(scores, axis=0, keepdims=True))
            weights = jnp.exp2(scores * score_base2 - after * score_base2)
            factor = jnp.exp2((before - after) * score_base2)
            total[group, head] = total[group, head] * factor + jnp.sum(weights, axis=0, keepdims=True)
            acc[group, head] = acc[group, head] * factor + jnp.dot(
                values_t[head * VDIM:(head + 1) * VDIM, :], weights.astype(jnp.bfloat16),
                preferred_element_type=jnp.float32)
            top[group, head] = after

    def process(block):
        @pl.when(block <= jnp.maximum(last_near, last_far))
        def _():
            expand(block)

        def one(group, carry):
            last = jnp.where(group == 0, last_near, last_far)

            @pl.when(block < last)
            def _():
                fold(group, False)

            @pl.when(block == last)
            def _():
                fold(group, True)

            return carry

        lax.fori_loop(0, 2, one, 0)

    def advance(place, carry):
        @pl.when(place == 1)
        def _():
            wait_received(0)
            start_phase(1)
            for at in (1, 2, 3, 4):
                pair_copy(at).start()

        @pl.when(place == 3)
        def _():
            wait_some(1, 0, 4)
            start_phase(2)
            for at in (5, 6):
                pair_copy(at).start()

        @pl.when(place == 5)
        def _():
            wait_some(1, 4, 12)
            start_phase(3)
            for at in (7, 8, 9, 10):
                pair_copy(at).start()

        @pl.when(place == 7)
        def _():
            out_wait(0)
            out_wait(1)
            for number in (3, 4, 5, 6):
                out_copy(*out_sends[number]).start()

        @pl.when(place == 8)
        def _():
            wait_received(2)
            wait_received(3)
            start_phase(4)
            for at in (11, 12, 13, 14):
                pair_copy(at).start()

        @pl.when(place == 13)
        def _():
            wait_received(4)
            pair_copy(15).start()
            out_wait(3)
            out_wait(4)
            out_copy(*out_sends[7]).start()

        dy = pick(place, [pair[0] for pair in ORDER])
        dz = pick(place, [pair[1] for pair in ORDER])
        base = 2 * sp_at(dy, dz)

        def plane(turn, carry):
            block = base + (core + turn) % 2

            @pl.when(turn == 1)
            def _():
                pltpu.make_async_remote_copy(
                    lat.at[block], lat.at[block], pair_send.at[place], pair_recv.at[place],
                    device_id=(s, partner), device_id_type=MESH).wait_recv()

            process(block)
            return carry

        lax.fori_loop(0, 2, plane, 0)
        return carry

    def wait_some(phase, first_index, last_index):
        for source, (first, count), step, slot in SENDS[phase][first_index:last_index]:
            place = at_receiver(source, step)
            block = relative(ORDER[place], core)
            pltpu.make_async_remote_copy(
                lat.at[block, pl.ds(first, count)], lat.at[block, pl.ds(first, count)],
                send_sem.at[0], recv_sem.at[4 * place + slot],
                device_id=(sp_at(*step), t), device_id_type=MESH).wait_recv()

    lax.fori_loop(0, 16, advance, 0)

    for group in range(2):
        for head in range(2):
            mixed = acc[group, head] / total[group, head]
            head_out[group, :, head * VDIM:(head + 1) * VDIM] = jnp.transpose(mixed).astype(jnp.bfloat16)

    def head_copy(group, part):
        target = part if group == 0 else 4 + part
        return pltpu.make_async_remote_copy(
            head_out.at[group, pl.ds(128 * part, 128)], heads_all.at[t],
            head_send.at[4 * group + part], head_recv.at[t],
            device_id=(s if group == 0 else mirror, target), device_id_type=MESH)

    for part in range(4):
        head_copy(1, part).start()

        @pl.when(t != part)
        def _():
            head_copy(0, part).start()

    @pl.when(t < 4)
    def _():
        mine = pltpu.make_async_copy(
            head_out.at[0, pl.ds(128 * (t % 4), 128)], heads_all.at[t], local_sem.at[2])
        mine.start()
        mine.wait()

    def head_wait(slot, carry):
        @pl.when((t >= 4) | (slot != t))
        def _():
            pltpu.make_async_remote_copy(
                head_out.at[0, pl.ds(0, 128)], heads_all.at[slot], head_send.at[0], head_recv.at[slot],
                device_id=(mirror, t), device_id_type=MESH).wait_recv()

        return carry

    lax.fori_loop(0, 8, head_wait, 0)

    own_out.wait()
    for number in (2, 5, 6, 7):
        out_wait(number)
    for number in range(8):
        out_copy(*out_sends[number]).wait_send()
    for copy in query_copies():
        copy.wait_send()
    for phase in range(len(SENDS)):
        for index in range(len(SENDS[phase])):
            shard_copy(phase, index).wait_send()
    for place in range(16):
        pair_copy(place).wait_send()
    for part in range(4):
        head_copy(1, part).wait_send()

        @pl.when(t != part)
        def _():
            head_copy(0, part).wait_send()


def attention_call(nope, rope, shard, w_key, w_value, w_out):
    vmem = pl.BlockSpec(memory_space=pltpu.VMEM)
    anywhere = pl.BlockSpec(memory_space=pl.ANY)
    dma = pltpu.SemaphoreType.DMA
    bf16, f32 = jnp.bfloat16, jnp.float32
    return pl.pallas_call(
        attention_kernel,
        out_shape=(
            jax.ShapeDtypeStruct((8, 128, 256), bf16),
            jax.ShapeDtypeStruct((8, 256, 2048), bf16),
        ),
        in_specs=[vmem] * 5 + [anywhere],
        out_specs=[anywhere, anywhere],
        scratch_shapes=[
            pltpu.VMEM((32, SHARD, 256), bf16),
            pltpu.VMEM((HALF, 256), bf16),
            pltpu.VMEM((HALF, 128), bf16),
            pltpu.VMEM((2, 2, 2, HALF, 256), bf16),
            pltpu.VMEM((2, HALF, 256), bf16),
            pltpu.VMEM((256, HALF), bf16),
            pltpu.VMEM((256, 256), bf16),
            pltpu.VMEM((2, 2, 1, HALF), f32),
            pltpu.VMEM((2, 2, 1, HALF), f32),
            pltpu.VMEM((2, 2, VDIM, HALF), f32),
            pltpu.VMEM((2, HALF, 256), bf16),
            dma((32,)), dma((64,)), dma((16,)), dma((16,)), dma((2,)), dma((2,)), dma((8,)), dma((8,)),
            dma((8,)), dma((8,)), dma((3,)),
        ],
        compiler_params=pltpu.CompilerParams(
            collective_id=0, has_side_effects=True, vmem_limit_bytes=48 * 1024 * 1024),
        cost_estimate=pl.CostEstimate(flops=60_000_000_000, bytes_accessed=30_000_000, transcendentals=18_000_000),
        name="attention",
    )(nope, rope, shard, w_key, w_value, w_out)


def rotate(values_in, cosine, sine_part):
    half_width = values_in.shape[-1] // 2
    front_half = values_in[..., :half_width]
    back_half = values_in[..., half_width:]
    return jnp.concatenate(
        [front_half * cosine - back_half * sine_part, back_half * cosine + front_half * sine_part],
        axis=-1,
    )


def angles(positions, full_width):
    half_width = full_width // 2
    frequency = theta_base ** (-2.0 * jnp.arange(half_width).astype(jnp.float32) / full_width)
    return positions[:, None] * frequency[None, :]


def rms_scale(values_in, gain):
    return (
        values_in
        * lax.rsqrt(jnp.mean(values_in * values_in, axis=-1, keepdims=True) + norm_eps)
        * gain
    )


def on_device(
    resid, query_nope, query_rope, latent, key_rope, latent_gain, w_key, w_value, w_out, mix_gain,
    w_gate, w_up, w_down,
):
    gate_full = lax.all_gather(w_gate, "sp", axis=0, tiled=True)
    up_full = lax.all_gather(w_up, "sp", axis=0, tiled=True)
    down_full = lax.all_gather(w_down, "sp", axis=0, tiled=True)

    core = lax.axis_index("tp") % 2
    first_row = lax.axis_index("sp") * ROWS
    angle = angles((first_row + jnp.arange(ROWS, dtype=jnp.int32)).astype(jnp.float32), ROPE)
    cosine, sine_part = jnp.cos(angle), jnp.sin(angle)
    rope_query = rotate(
        query_rope.astype(jnp.float32).reshape(ROWS, 2, ROPE), cosine[:, None, :], sine_part[:, None, :]
    ).astype(jnp.bfloat16).reshape(ROWS, 2 * ROPE)

    def my_half(array):
        return lax.dynamic_slice_in_dim(array, core * HALF, HALF, 0)

    latent_normed = rms_scale(my_half(latent).astype(jnp.float32), latent_gain).astype(jnp.bfloat16)
    key_rotated = rotate(my_half(key_rope).astype(jnp.float32), my_half(cosine), my_half(sine_part)).astype(jnp.bfloat16)
    quarters = key_rotated.reshape(4, 128, ROPE)
    packed = jnp.concatenate([quarters[0], quarters[2], quarters[1], quarters[3]], axis=1)
    shard = jnp.concatenate([latent_normed, packed], axis=0)

    heads_all, w_out_all = attention_call(query_nope, rope_query, shard, w_key, w_value, w_out)
    attention_proj = jnp.einsum("gtv,gvd->td", heads_all, w_out_all, preferred_element_type=jnp.float32)
    stream = resid.astype(jnp.float32) + attention_proj
    normed = rms_scale(stream, mix_gain).astype(jnp.bfloat16)
    row_piece = lax.all_gather(normed, "tp", axis=0, tiled=True)
    gate_value = jnp.dot(row_piece, gate_full, preferred_element_type=jnp.float32)
    upward = jnp.dot(row_piece, up_full, preferred_element_type=jnp.float32)
    hidden = (jax.nn.silu(gate_value) * upward).astype(jnp.bfloat16)
    down_term = lax.dot_general(
        hidden, down_full, (((1,), (1,)), ((), ())), preferred_element_type=jnp.float32
    ).astype(jnp.bfloat16)
    mixer_out = lax.psum_scatter(down_term, "tp", scatter_dimension=0, tiled=True).astype(jnp.float32)
    return (stream + 0.5 * mixer_out).astype(jnp.bfloat16)


def solution(mesh):
    return jax.shard_map(
        on_device,
        mesh=mesh,
        in_specs=(
            P(("sp", "tp"), None),
            P("sp", "tp"),
            P("sp", "tp"),
            P("sp", None),
            P("sp", None),
            P(),
            P(None, "tp"),
            P(None, "tp"),
            P("tp", None),
            P(),
            P("sp", "tp"),
            P("sp", "tp"),
            P("sp", "tp"),
        ),
        out_specs=P(("sp", "tp"), None),
        check_vma=False,
    )
```

```python
import functools

import jax
import jax.numpy as jnp
from jax import lax
from jax.experimental import pallas as pl
from jax.experimental.pallas import tpu as pltpu
from jax.sharding import PartitionSpec as P

NOPE = 128
ROPE = 64
VDIM = 128
ROWS = 1024
HALF = 512
SIDE = 4
SHARD = HALF + HALF // 4

norm_eps = 1e-06
masked_score = -1e30
theta_base = 10000.0
score_base2 = (NOPE + ROPE) ** (-0.5) * 1.4426950408889634
MESH = pl.DeviceIdType.MESH

ORDER = ((0, 0), (1, 0), (3, 0), (0, 1), (0, 3), (2, 0), (0, 2), (1, 1), (1, 3), (3, 1), (3, 3),
         (2, 1), (2, 3), (1, 2), (3, 2), (2, 2))
PLACE = {pair: p for p, pair in enumerate(ORDER)}
ALPHA, BETA, FULL = (0, 320), (320, 320), (0, 640)
ALPHA0, ALPHA1, BETA0, BETA1 = (0, 160), (160, 160), (320, 160), (480, 160)

SENDS = (
    (((0, 0), FULL, (1, 0), 0), ((0, 0), FULL, (-1, 0), 0), ((0, 0), FULL, (0, 1), 0), ((0, 0), FULL, (0, -1), 0)),
    (
        ((1, 0), ALPHA, (-1, 0), 0), ((3, 0), BETA, (1, 0), 1),
        ((0, 1), ALPHA, (0, -1), 0), ((0, 3), BETA, (0, 1), 1),
        ((1, 0), ALPHA, (0, 1), 0), ((1, 0), ALPHA, (0, -1), 0),
        ((3, 0), ALPHA, (0, 1), 0), ((3, 0), ALPHA, (0, -1), 0),
        ((0, 1), BETA, (1, 0), 1), ((0, 1), BETA, (-1, 0), 1),
        ((0, 3), BETA, (1, 0), 1), ((0, 3), BETA, (-1, 0), 1),
    ),
    (
        ((2, 0), ALPHA, (0, 1), 0), ((2, 0), ALPHA, (0, -1), 0),
        ((0, 2), BETA, (1, 0), 1), ((0, 2), BETA, (-1, 0), 1),
    ),
    (
        ((1, 1), ALPHA0, (0, -1), 0), ((1, 3), ALPHA1, (0, 1), 2),
        ((3, 1), ALPHA0, (0, -1), 0), ((3, 3), ALPHA1, (0, 1), 2),
        ((1, 1), BETA0, (-1, 0), 1), ((3, 1), BETA1, (1, 0), 2),
        ((1, 3), BETA0, (-1, 0), 1), ((3, 3), BETA1, (1, 0), 2),
    ),
    (
        ((2, 1), ALPHA0, (0, -1), 0), ((2, 3), ALPHA1, (0, 1), 1),
        ((1, 2), BETA0, (-1, 0), 2), ((3, 2), BETA1, (1, 0), 3),
    ),
)


def at_receiver(source, step):
    return PLACE[((source[0] - step[0]) % SIDE, (source[1] - step[1]) % SIDE)]


def pick(index, values):
    found = jnp.int32(values[0])
    for at in range(1, len(values)):
        found = jnp.where(index == at, jnp.int32(values[at]), found)
    return found


def layer_kernel(
    nope, rope, shard, w_key, w_value, w_out, mixer, resid, mix_gain, result,
    lat, far_nope, far_rope, queries, keys, values_t, w_value_t, top, total, acc, head_out,
    heads_all, w_out_all, weights_all, stream, rows_all, halves, got, summed, relay, arrived,
    send_sem, recv_sem, pair_send, pair_recv, query_send, query_recv, head_send, head_recv,
    out_send, out_recv, local_sem, mixer_send, mixer_recv, row_send, row_recv, part_send, part_recv,
    sum_send, sum_recv,
):
    s = lax.axis_index("sp")
    t = lax.axis_index("tp")
    z, y = s // SIDE, s % SIDE
    x, core = t // 2, t % 2
    mirror = 15 - s

    def sp_at(dy, dz):
        return ((z + dz + SIDE) % SIDE) * SIDE + (y + dy + SIDE) % SIDE

    def tp_at(dx):
        return ((x + dx + SIDE) % SIDE) * 2 + core

    partner = x * 2 + 1 - core

    barrier = pltpu.get_barrier_semaphore()
    for step in (1, 2, 3):
        pl.semaphore_signal(barrier, inc=1, device_id=(sp_at(step, 0), t), device_id_type=MESH)
        pl.semaphore_signal(barrier, inc=1, device_id=(sp_at(0, step), t), device_id_type=MESH)
    for step in range(1, 8):
        pl.semaphore_signal(barrier, inc=1, device_id=(s, (t + step) % 8), device_id_type=MESH)
    for step in range(8):
        pl.semaphore_signal(barrier, inc=1, device_id=(mirror, (t + step) % 8), device_id_type=MESH)
    pl.semaphore_wait(barrier, 21)

    def query_copies():
        return (
            pltpu.make_async_remote_copy(
                nope.at[pl.ds(HALF, HALF)], far_nope, query_send.at[0], query_recv.at[0],
                device_id=(mirror, t), device_id_type=MESH),
            pltpu.make_async_remote_copy(
                rope.at[pl.ds(HALF, HALF)], far_rope, query_send.at[1], query_recv.at[1],
                device_id=(mirror, t), device_id_type=MESH),
        )

    for copy in query_copies():
        copy.start()

    own = 2 * s + core

    def piece(kind, block, rows):
        first, count = rows
        if kind == 0:
            return lat.at[2 * block + core, pl.ds(first, count)]
        return weights_all.at[pl.ds(128 * block + first // 5, count // 5)]

    def shard_copy(kind, phase, index):
        source, rows, step, slot = SENDS[phase][index]
        number = sum(len(one) for one in SENDS[:phase]) + index
        place = at_receiver(source, step)
        there = piece(kind, sp_at(*source), rows)
        if phase > 0:
            here = there
        else:
            here = shard if kind == 0 else mixer
        return pltpu.make_async_remote_copy(
            here, there,
            (send_sem, mixer_send)[kind].at[number], (recv_sem, mixer_recv)[kind].at[4 * place + slot],
            device_id=(sp_at(*step), t), device_id_type=MESH)

    def start_phase(kind, phase):
        for index in range(len(SENDS[phase])):
            shard_copy(kind, phase, index).start()

    def wait_received(kind, phase, first_index=0, last_index=12):
        for source, rows, step, slot in SENDS[phase][first_index:last_index]:
            place = at_receiver(source, step)
            there = piece(kind, sp_at(*ORDER[place]), rows)
            pltpu.make_async_remote_copy(
                there, there,
                (send_sem, mixer_send)[kind].at[0], (recv_sem, mixer_recv)[kind].at[4 * place + slot],
                device_id=(sp_at(*step), t), device_id_type=MESH).wait_recv()

    def pair_copy(place):
        block = 2 * sp_at(*ORDER[place]) + core
        return pltpu.make_async_remote_copy(
            shard if place == 0 else lat.at[block], lat.at[block],
            pair_send.at[place], pair_recv.at[place],
            device_id=(s, partner), device_id_type=MESH)

    def out_copy(number, slot, rows, target):
        first, count = rows
        source = w_out.at[pl.ds(first, count)] if number < 3 else w_out_all.at[slot, pl.ds(first, count)]
        return pltpu.make_async_remote_copy(
            source, w_out_all.at[slot, pl.ds(first, count)],
            out_send.at[number], out_recv.at[number],
            device_id=(s, target), device_id_type=MESH)

    whole, upper, lower = (0, 256), (0, 128), (128, 128)
    right, left, across = tp_at(1), tp_at(3), tp_at(2)
    out_sends = (
        (0, t, whole, right), (1, t, whole, left), (2, t, whole, partner),
        (3, right, upper, left), (4, left, lower, right),
        (5, right, whole, partner), (6, left, whole, partner), (7, across, whole, partner),
    )

    def other(slot):
        return (slot // 2) * 2 + 1 - slot % 2

    out_receives = (
        (0, left, whole), (1, right, whole), (2, partner, whole),
        (3, across, upper), (4, across, lower),
        (5, other(right), whole), (6, other(left), whole), (7, other(across), whole),
    )

    def out_wait(number):
        _, slot, (first, count) = out_receives[number]
        pltpu.make_async_remote_copy(
            w_out_all.at[slot, pl.ds(first, count)], w_out_all.at[slot, pl.ds(first, count)],
            out_send.at[number], out_recv.at[number],
            device_id=(s, partner), device_id_type=MESH).wait_recv()

    start_phase(0, 0)
    pair_copy(0).start()
    for number in range(3):
        out_copy(*out_sends[number]).start()
    own_shard = pltpu.make_async_copy(shard, lat.at[own], local_sem.at[0])
    own_shard.start()
    own_out = pltpu.make_async_copy(w_out, w_out_all.at[t], local_sem.at[1])
    own_out.start()
    own_mixer = pltpu.make_async_copy(mixer, weights_all.at[pl.ds(128 * s, 128)], local_sem.at[3])
    own_mixer.start()

    w_value_t[...] = jnp.transpose(w_value[...].astype(jnp.float32)).astype(jnp.bfloat16)
    top[...] = jnp.full_like(top, masked_score)
    total[...] = jnp.zeros_like(total)
    acc[...] = jnp.zeros_like(acc)

    lanes = lax.broadcasted_iota(jnp.int32, (HALF, 128), 1)

    def set_queries(group, nope_rows, rope_rows):
        wide = rope_rows.astype(jnp.float32)
        turned = pltpu.roll(wide, 64, 1)
        front = lanes < 64
        for head in range(2):
            one = nope_rows[:, head * NOPE:(head + 1) * NOPE]
            low, high = (wide, turned) if head == 0 else (turned, wide)
            for version, tail in enumerate((jnp.where(front, low, 0.0), jnp.where(front, 0.0, high))):
                queries[group, head, version, :, 0:NOPE] = one
                queries[group, head, version, :, NOPE:2 * NOPE] = tail.astype(jnp.bfloat16)

    set_queries(0, nope[pl.ds(0, HALF), :], rope[pl.ds(0, HALF), :])
    own_shard.wait()
    for copy in query_copies():
        copy.wait_recv()
    set_queries(1, far_nope[...], far_rope[...])

    last_near, last_far = 2 * s, 31 - 2 * s

    def expand(block):
        rows = lat[block, pl.ds(0, HALF), :]
        expanded = jnp.dot(rows, w_key[...], preferred_element_type=jnp.float32).astype(jnp.bfloat16)
        tails = (lat[block, pl.ds(HALF, 128), 0:128], lat[block, pl.ds(HALF, 128), 128:256])
        for head in range(2):
            keys[head, :, 0:NOPE] = expanded[:, head * NOPE:(head + 1) * NOPE]
            for quarter in range(4):
                keys[head, pl.ds(quarter * 128, 128), NOPE:2 * NOPE] = tails[quarter % 2]
        values_t[...] = lax.dot_general(
            w_value_t[...], rows, (((1,), (1,)), ((), ())), preferred_element_type=jnp.float32
        ).astype(jnp.bfloat16)

    def fold(group, masked):
        for head in range(2):
            scores = jnp.concatenate(
                [
                    lax.dot_general(
                        keys[head, pl.ds(256 * version, 256), :], queries[group, head, version],
                        (((1,), (1,)), ((), ())), preferred_element_type=jnp.float32)
                    for version in range(2)
                ],
                axis=0,
            )
            if masked:
                key_at = lax.broadcasted_iota(jnp.int32, scores.shape, 0)
                query_at = lax.broadcasted_iota(jnp.int32, scores.shape, 1)
                scores = jnp.where(key_at <= query_at, scores, masked_score)
            before = top[group, head]
            after = jnp.maximum(before, jnp.max(scores, axis=0, keepdims=True))
            weights = jnp.exp2(scores * score_base2 - after * score_base2)
            factor = jnp.exp2((before - after) * score_base2)
            total[group, head] = total[group, head] * factor + jnp.sum(weights, axis=0, keepdims=True)
            acc[group, head] = acc[group, head] * factor + jnp.dot(
                values_t[head * VDIM:(head + 1) * VDIM, :], weights.astype(jnp.bfloat16),
                preferred_element_type=jnp.float32)
            top[group, head] = after

    def process(block):
        @pl.when(block <= jnp.maximum(last_near, last_far))
        def _():
            expand(block)

        def one(group, carry):
            last = jnp.where(group == 0, last_near, last_far)

            @pl.when(block < last)
            def _():
                fold(group, False)

            @pl.when(block == last)
            def _():
                fold(group, True)

            return carry

        lax.fori_loop(0, 2, one, 0)

    def advance(place, carry):
        @pl.when(place == 1)
        def _():
            wait_received(0, 0)
            start_phase(0, 1)
            for at in (1, 2, 3, 4):
                pair_copy(at).start()
            start_phase(1, 0)

        @pl.when(place == 3)
        def _():
            wait_received(0, 1, 0, 4)
            start_phase(0, 2)
            for at in (5, 6):
                pair_copy(at).start()

        @pl.when(place == 5)
        def _():
            wait_received(0, 1, 4, 12)
            start_phase(0, 3)
            for at in (7, 8, 9, 10):
                pair_copy(at).start()

        @pl.when(place == 7)
        def _():
            out_wait(0)
            out_wait(1)
            for number in (3, 4, 5, 6):
                out_copy(*out_sends[number]).start()

        @pl.when(place == 8)
        def _():
            wait_received(0, 2)
            wait_received(0, 3)
            start_phase(0, 4)
            for at in (11, 12, 13, 14):
                pair_copy(at).start()
            wait_received(1, 0)
            start_phase(1, 1)

        @pl.when(place == 12)
        def _():
            wait_received(0, 4)
            pair_copy(15).start()
            out_wait(3)
            out_wait(4)
            out_copy(*out_sends[7]).start()
            wait_received(1, 1, 0, 4)
            start_phase(1, 2)

        dy = pick(place, [pair[0] for pair in ORDER])
        dz = pick(place, [pair[1] for pair in ORDER])
        base = 2 * sp_at(dy, dz)

        def plane(turn, carry):
            block = base + (core + turn) % 2

            @pl.when(turn == 1)
            def _():
                pltpu.make_async_remote_copy(
                    lat.at[block], lat.at[block], pair_send.at[place], pair_recv.at[place],
                    device_id=(s, partner), device_id_type=MESH).wait_recv()

            process(block)
            return carry

        lax.fori_loop(0, 2, plane, 0)
        return carry

    lax.fori_loop(0, 16, advance, 0)

    for group in range(2):
        for head in range(2):
            mixed = acc[group, head] / total[group, head]
            head_out[group, :, head * VDIM:(head + 1) * VDIM] = jnp.transpose(mixed).astype(jnp.bfloat16)

    def head_copy(group, part):
        target = part if group == 0 else 4 + part
        return pltpu.make_async_remote_copy(
            head_out.at[group, pl.ds(128 * part, 128)], heads_all.at[t],
            head_send.at[4 * group + part], head_recv.at[t],
            device_id=(s if group == 0 else mirror, target), device_id_type=MESH)

    for part in range(4):
        head_copy(1, part).start()

        @pl.when(t != part)
        def _():
            head_copy(0, part).start()

    @pl.when(t < 4)
    def _():
        mine = pltpu.make_async_copy(
            head_out.at[0, pl.ds(128 * (t % 4), 128)], heads_all.at[t], local_sem.at[2])
        mine.start()
        mine.wait()

    wait_received(1, 1, 4, 12)
    start_phase(1, 3)

    def head_wait(slot, carry):
        @pl.when((t >= 4) | (slot != t))
        def _():
            pltpu.make_async_remote_copy(
                head_out.at[0, pl.ds(0, 128)], heads_all.at[slot], head_send.at[0], head_recv.at[slot],
                device_id=(mirror, t), device_id_type=MESH).wait_recv()

        return carry

    own_out.wait()
    for number in (2, 5, 6, 7):
        out_wait(number)
    lax.fori_loop(0, 8, head_wait, 0)

    stream[...] = resid[...].astype(jnp.float32)

    def project(slot, carry):
        stream[...] += jnp.dot(heads_all[slot], w_out_all[slot], preferred_element_type=jnp.float32)
        return carry

    lax.fori_loop(0, 8, project, 0)
    rows_f32 = stream[...]
    scale = lax.rsqrt(jnp.mean(rows_f32 * rows_f32, axis=-1, keepdims=True) + norm_eps)
    rows_all[t] = (rows_f32 * scale * mix_gain[...]).astype(jnp.bfloat16)

    high, low = (0, 64), (64, 64)
    all_rows = (0, 128)
    row_sends = (
        (0, t, all_rows, right), (1, t, all_rows, left), (2, t, all_rows, partner),
        (3, right, high, left), (4, left, low, right),
        (5, right, all_rows, partner), (6, left, all_rows, partner), (7, across, all_rows, partner),
    )
    row_receives = (
        (0, left, all_rows), (1, right, all_rows), (2, partner, all_rows),
        (3, across, high), (4, across, low),
        (5, other(right), all_rows), (6, other(left), all_rows), (7, other(across), all_rows),
    )

    def row_copy(number):
        _, slot, (first, count), target = row_sends[number]
        here = rows_all.at[slot, pl.ds(first, count)]
        return pltpu.make_async_remote_copy(
            here, here, row_send.at[number], row_recv.at[number],
            device_id=(s, target), device_id_type=MESH)

    def row_wait(number):
        _, slot, (first, count) = row_receives[number]
        here = rows_all.at[slot, pl.ds(first, count)]
        pltpu.make_async_remote_copy(
            here, here, row_send.at[number], row_recv.at[number],
            device_id=(s, partner), device_id_type=MESH).wait_recv()

    for number in range(3):
        row_copy(number).start()

    wait_received(1, 2)
    wait_received(1, 3)
    start_phase(1, 4)
    own_mixer.wait()
    row_wait(0)
    row_wait(1)
    for number in (3, 4, 5, 6):
        row_copy(number).start()
    wait_received(1, 4)

    def part_copy(step):
        return pltpu.make_async_remote_copy(
            halves.at[step, 1 - core], got.at[step], part_send.at[step], part_recv.at[step],
            device_id=(s, partner), device_id_type=MESH)

    def chip_total(step):
        part_copy(step).wait_recv()
        return halves[step, core].astype(jnp.float32) + got[step].astype(jnp.float32)

    def sum_copy(number):
        here, there, target = (
            (summed.at[1], arrived.at[0], right),
            (summed.at[2], arrived.at[1], left),
            (summed.at[3, pl.ds(0, 64)], relay.at[0], right),
            (summed.at[3, pl.ds(64, 64)], relay.at[1], left),
            (relay.at[0], arrived.at[2, pl.ds(0, 64)], right),
            (relay.at[1], arrived.at[2, pl.ds(64, 64)], left),
        )[number]
        return pltpu.make_async_remote_copy(
            here, there, sum_send.at[number], sum_recv.at[number],
            device_id=(s, target), device_id_type=MESH)

    def mix(step, carry):
        @pl.when(step == 0)
        def _():
            row_wait(2)

        @pl.when(step == 1)
        def _():
            row_wait(5)
            row_wait(6)

        @pl.when(step == 2)
        def _():
            row_wait(3)
            row_wait(4)
            row_copy(7).start()

        @pl.when(step == 3)
        def _():
            row_wait(7)

        chip = (x + pick(step, (0, 1, 3, 2))) % SIDE
        rows = rows_all[pl.ds(2 * chip, 2)].reshape(256, 2048)
        both = jnp.dot(rows, weights_all[:, 0:1408], preferred_element_type=jnp.float32)
        gate_value, upward = both[:, 0:704], both[:, 704:1408]
        hidden = (gate_value / (1.0 + jnp.exp(-gate_value)) * upward).astype(jnp.bfloat16)
        down = lax.dot_general(
            hidden, weights_all[:, 1408:2112], (((1,), (1,)), ((), ())), preferred_element_type=jnp.float32)
        halves[step] = down.astype(jnp.bfloat16).reshape(2, 128, 2048)
        part_copy(step).start()

        @pl.when(step == 1)
        def _():
            stream[...] += 0.5 * chip_total(0)

        @pl.when(step == 2)
        def _():
            summed[1] = chip_total(1).astype(jnp.bfloat16)
            sum_copy(0).start()

        @pl.when(step == 3)
        def _():
            summed[2] = chip_total(2).astype(jnp.bfloat16)
            sum_copy(1).start()

        return carry

    lax.fori_loop(0, 4, mix, 0)
    summed[3] = chip_total(3).astype(jnp.bfloat16)
    sum_copy(2).start()
    sum_copy(3).start()
    sum_copy(2).wait_recv()
    sum_copy(4).start()
    sum_copy(3).wait_recv()
    sum_copy(5).start()
    sum_copy(0).wait_recv()
    sum_copy(1).wait_recv()
    stream[...] += 0.5 * (arrived[0].astype(jnp.float32) + arrived[1].astype(jnp.float32))
    sum_copy(4).wait_recv()
    sum_copy(5).wait_recv()
    result[...] = (stream[...] + 0.5 * arrived[2].astype(jnp.float32)).astype(jnp.bfloat16)

    for number in range(6):
        sum_copy(number).wait_send()
    for step in range(4):
        part_copy(step).wait_send()
    for number in range(8):
        row_copy(number).wait_send()
        out_copy(*out_sends[number]).wait_send()
    for copy in query_copies():
        copy.wait_send()
    for phase in range(len(SENDS)):
        for index in range(len(SENDS[phase])):
            shard_copy(0, phase, index).wait_send()
            shard_copy(1, phase, index).wait_send()
    for place in range(16):
        pair_copy(place).wait_send()
    for number in range(4):
        head_copy(1, number).wait_send()

        @pl.when(t != number)
        def _():
            head_copy(0, number).wait_send()


def layer_call(nope, rope, shard, w_key, w_value, w_out, mixer, resid, mix_gain):
    vmem = pl.BlockSpec(memory_space=pltpu.VMEM)
    anywhere = pl.BlockSpec(memory_space=pl.ANY)
    dma = pltpu.SemaphoreType.DMA
    bf16, f32 = jnp.bfloat16, jnp.float32
    return pl.pallas_call(
        layer_kernel,
        out_shape=jax.ShapeDtypeStruct((128, 2048), bf16),
        in_specs=[vmem] * 5 + [anywhere, anywhere, vmem, vmem],
        out_specs=vmem,
        scratch_shapes=[
            pltpu.VMEM((32, SHARD, 256), bf16),
            pltpu.VMEM((HALF, 256), bf16),
            pltpu.VMEM((HALF, 128), bf16),
            pltpu.VMEM((2, 2, 2, HALF, 256), bf16),
            pltpu.VMEM((2, HALF, 256), bf16),
            pltpu.VMEM((256, HALF), bf16),
            pltpu.VMEM((256, 256), bf16),
            pltpu.VMEM((2, 2, 1, HALF), f32),
            pltpu.VMEM((2, 2, 1, HALF), f32),
            pltpu.VMEM((2, 2, VDIM, HALF), f32),
            pltpu.VMEM((2, HALF, 256), bf16),
            pltpu.VMEM((8, 128, 256), bf16),
            pltpu.VMEM((8, 256, 2048), bf16),
            pltpu.VMEM((2048, 2112), bf16),
            pltpu.VMEM((128, 2048), f32),
            pltpu.VMEM((8, 128, 2048), bf16),
            pltpu.VMEM((4, 2, 128, 2048), bf16),
            pltpu.VMEM((4, 128, 2048), bf16),
            pltpu.VMEM((4, 128, 2048), bf16),
            pltpu.VMEM((2, 64, 2048), bf16),
            pltpu.VMEM((3, 128, 2048), bf16),
            dma((32,)), dma((64,)), dma((16,)), dma((16,)), dma((2,)), dma((2,)), dma((8,)), dma((8,)),
            dma((8,)), dma((8,)), dma((4,)),
            dma((32,)), dma((64,)), dma((8,)), dma((8,)), dma((4,)), dma((4,)), dma((6,)), dma((6,)),
        ],
        compiler_params=pltpu.CompilerParams(
            collective_id=0, has_side_effects=True, vmem_limit_bytes=67_000_000),
        cost_estimate=pl.CostEstimate(flops=60_000_000_000, bytes_accessed=30_000_000, transcendentals=18_000_000),
        name="layer",
    )(nope, rope, shard, w_key, w_value, w_out, mixer, resid, mix_gain)


def rotate(values_in, cosine, sine_part):
    half_width = values_in.shape[-1] // 2
    front_half = values_in[..., :half_width]
    back_half = values_in[..., half_width:]
    return jnp.concatenate(
        [front_half * cosine - back_half * sine_part, back_half * cosine + front_half * sine_part],
        axis=-1,
    )


def angles(positions, full_width):
    half_width = full_width // 2
    frequency = theta_base ** (-2.0 * jnp.arange(half_width).astype(jnp.float32) / full_width)
    return positions[:, None] * frequency[None, :]


def rms_scale(values_in, gain):
    return (
        values_in
        * lax.rsqrt(jnp.mean(values_in * values_in, axis=-1, keepdims=True) + norm_eps)
        * gain
    )


def on_device(
    resid, query_nope, query_rope, latent, key_rope, latent_gain, w_key, w_value, w_out, mix_gain,
    w_gate, w_up, w_down,
):
    core = lax.axis_index("tp") % 2
    first_row = lax.axis_index("sp") * ROWS
    angle = angles((first_row + jnp.arange(ROWS, dtype=jnp.int32)).astype(jnp.float32), ROPE)
    cosine, sine_part = jnp.cos(angle), jnp.sin(angle)
    rope_query = rotate(
        query_rope.astype(jnp.float32).reshape(ROWS, 2, ROPE), cosine[:, None, :], sine_part[:, None, :]
    ).astype(jnp.bfloat16).reshape(ROWS, 2 * ROPE)

    def my_half(array):
        return lax.dynamic_slice_in_dim(array, core * HALF, HALF, 0)

    latent_normed = rms_scale(my_half(latent).astype(jnp.float32), latent_gain).astype(jnp.bfloat16)
    key_rotated = rotate(my_half(key_rope).astype(jnp.float32), my_half(cosine), my_half(sine_part)).astype(jnp.bfloat16)
    quarters = key_rotated.reshape(4, 128, ROPE)
    packed = jnp.concatenate([quarters[0], quarters[2], quarters[1], quarters[3]], axis=1)
    shard = jnp.concatenate([latent_normed, packed], axis=0)

    mixer = jnp.concatenate([w_gate, w_up, w_down], axis=1)
    return layer_call(
        query_nope, rope_query, shard, w_key, w_value, w_out, mixer, resid, mix_gain.reshape(1, -1))


def solution(mesh):
    return jax.shard_map(
        on_device,
        mesh=mesh,
        in_specs=(
            P(("sp", "tp"), None),
            P("sp", "tp"),
            P("sp", "tp"),
            P("sp", None),
            P("sp", None),
            P(),
            P(None, "tp"),
            P(None, "tp"),
            P("tp", None),
            P(),
            P("sp", "tp"),
            P("sp", "tp"),
            P("sp", "tp"),
        ),
        out_specs=P(("sp", "tp"), None),
        check_vma=False,
    )
```

```python
import functools

import jax
import jax.numpy as jnp
import numpy as np
from jax import lax
from jax.experimental import pallas as pl
from jax.experimental.pallas import tpu as pltpu
from jax.sharding import PartitionSpec as P

NOPE = 128
ROPE = 64
VDIM = 128
ROWS = 1024
HALF = 512
SIDE = 4
QUARTER = 256
UNITS = 704
SHARD = QUARTER + QUARTER // 4

norm_eps = 1e-06
masked_score = -1e30
theta_base = 10000.0
score_base2 = (NOPE + ROPE) ** (-0.5) * 1.4426950408889634
MESH = pl.DeviceIdType.MESH

ORDER = ((0, 0), (1, 0), (3, 0), (0, 1), (0, 3), (2, 0), (0, 2), (1, 1), (1, 3), (3, 1), (3, 3),
         (2, 1), (2, 3), (1, 2), (3, 2), (2, 2))
PLACE = {pair: p for p, pair in enumerate(ORDER)}
ALPHA, BETA, FULL = (0, 320), (320, 320), (0, 640)
ALPHA0, ALPHA1, BETA0, BETA1 = (0, 160), (160, 160), (320, 160), (480, 160)

SENDS = (
    (((0, 0), FULL, (1, 0), 0), ((0, 0), FULL, (-1, 0), 0), ((0, 0), FULL, (0, 1), 0), ((0, 0), FULL, (0, -1), 0)),
    (
        ((1, 0), ALPHA, (-1, 0), 0), ((3, 0), BETA, (1, 0), 1),
        ((0, 1), ALPHA, (0, -1), 0), ((0, 3), BETA, (0, 1), 1),
        ((1, 0), ALPHA, (0, 1), 0), ((1, 0), ALPHA, (0, -1), 0),
        ((3, 0), ALPHA, (0, 1), 0), ((3, 0), ALPHA, (0, -1), 0),
        ((0, 1), BETA, (1, 0), 1), ((0, 1), BETA, (-1, 0), 1),
        ((0, 3), BETA, (1, 0), 1), ((0, 3), BETA, (-1, 0), 1),
    ),
    (
        ((2, 0), ALPHA, (0, 1), 0), ((2, 0), ALPHA, (0, -1), 0),
        ((0, 2), BETA, (1, 0), 1), ((0, 2), BETA, (-1, 0), 1),
    ),
    (
        ((1, 1), ALPHA0, (0, -1), 0), ((1, 3), ALPHA1, (0, 1), 2),
        ((3, 1), ALPHA0, (0, -1), 0), ((3, 3), ALPHA1, (0, 1), 2),
        ((1, 1), BETA0, (-1, 0), 1), ((3, 1), BETA1, (1, 0), 2),
        ((1, 3), BETA0, (-1, 0), 1), ((3, 3), BETA1, (1, 0), 2),
    ),
    (
        ((2, 1), ALPHA0, (0, -1), 0), ((2, 3), ALPHA1, (0, 1), 1),
        ((1, 2), BETA0, (-1, 0), 2), ((3, 2), BETA1, (1, 0), 3),
    ),
)


def at_receiver(source, step):
    return PLACE[((source[0] - step[0]) % SIDE, (source[1] - step[1]) % SIDE)]


def pick(index, values):
    found = jnp.int32(values[0])
    for at in range(1, len(values)):
        found = jnp.where(index == at, jnp.int32(values[at]), found)
    return found


def layer_kernel(
    nope_in, rope_in, latent_in, key_in, gain_in, w_key_in, w_value_in, w_out, resid_in, mix_gain_in,
    gate_in, up_in, down_in, row_cos_in, row_sin_in, block_cos_in, block_sin_in, result,
    nope, rope, latent, key_rope, gain, w_key, w_value, resid, mix_gain,
    row_cos, row_sin, block_cos, block_sin, turned_queries,
    lat, far_nope, far_rope, queries, keys, values_t, held, w_value_t, top, total, acc, head_out,
    heads_all, w_out_all, weights_all, hidden, stream, rows_all, halves, got, summed, relay, arrived,
    send_sem, recv_sem, side_send, side_recv, pair_send, pair_recv, query_send, query_recv, head_send, head_recv,
    out_send, out_recv, local_sem, mixer_send, mixer_recv, row_send, row_recv, part_send, part_recv,
    sum_send, sum_recv, load_sem,
):
    s = lax.axis_index("sp")
    t = lax.axis_index("tp")
    z, y = s // SIDE, s % SIDE
    x, core = t // 2, t % 2
    mirror = 15 - s

    def sp_at(dy, dz):
        return ((z + dz + SIDE) % SIDE) * SIDE + (y + dy + SIDE) % SIDE

    def tp_at(dx):
        return ((x + dx + SIDE) % SIDE) * 2 + core

    partner = x * 2 + 1 - core
    mine = 2 * (x % 2) + core
    beside = 2 * (1 - x % 2) + core

    barrier = pltpu.get_barrier_semaphore()
    for step in (1, 2, 3):
        pl.semaphore_signal(barrier, inc=1, device_id=(sp_at(step, 0), t), device_id_type=MESH)
        pl.semaphore_signal(barrier, inc=1, device_id=(sp_at(0, step), t), device_id_type=MESH)
    for step in range(1, 8):
        pl.semaphore_signal(barrier, inc=1, device_id=(s, (t + step) % 8), device_id_type=MESH)
    for step in range(8):
        pl.semaphore_signal(barrier, inc=1, device_id=(mirror, (t + step) % 8), device_id_type=MESH)

    quarter_rows = pl.ds(pl.multiple_of((2 * (x % 2) + core) * QUARTER, QUARTER), QUARTER)
    loads = [
        pltpu.make_async_copy(source, target, load_sem.at[number])
        for number, (source, target) in enumerate((
            (latent_in.at[quarter_rows], latent), (key_in.at[:, quarter_rows], key_rope), (gain_in, gain),
            (block_cos_in, block_cos), (block_sin_in, block_sin), (row_cos_in, row_cos), (row_sin_in, row_sin),
            (rope_in, rope), (nope_in, nope), (w_value_in, w_value), (w_key_in, w_key),
            (gate_in, weights_all.at[s, pl.ds(0, UNITS)]), (up_in, weights_all.at[s, pl.ds(UNITS, UNITS)]),
            (down_in, weights_all.at[s, pl.ds(2 * UNITS, UNITS)]), (resid_in, resid), (mix_gain_in, mix_gain),
        ))
    ]
    for load in loads:
        load.start()

    def rotated(rows_in, first):
        count = rows_in.shape[0]
        at = pl.ds(first, count)
        near_cos, near_sin = row_cos[at, :], row_sin[at, :]
        far_cos, far_sin = block_cos[pl.ds(s, 1), :], block_sin[pl.ds(s, 1), :]
        cosine = far_cos * near_cos - far_sin * near_sin
        sine = far_sin * near_cos + far_cos * near_sin
        lane = lax.broadcasted_iota(jnp.int32, rows_in.shape, 1) % ROPE
        swapped = jnp.where(lane < ROPE // 2, -pltpu.roll(rows_in, 96, 1), pltpu.roll(rows_in, 32, 1))
        return rows_in * cosine + swapped * sine

    own = 4 * s + 2 * (x % 2) + core
    for load in loads[:7]:
        load.wait()
    wide = latent[...].astype(jnp.float32)
    scale = lax.rsqrt(jnp.mean(wide * wide, axis=-1, keepdims=True) + norm_eps)
    lat[own, pl.ds(0, QUARTER), :] = (wide * scale * gain[...]).astype(jnp.bfloat16)
    once = key_rope[...].astype(jnp.float32)
    twice = rotated(jnp.transpose(jnp.concatenate([once, once], axis=0)), (2 * (x % 2) + core) * QUARTER).astype(jnp.bfloat16)
    front_lanes = lax.broadcasted_iota(jnp.int32, (64, 128), 1) < ROPE
    for side in range(2):
        lat[own, pl.ds(QUARTER, 64), side * 128:(side + 1) * 128] = jnp.where(
            front_lanes, twice[64 * side:64 * side + 64], twice[128 + 64 * side:192 + 64 * side])
    for load in loads[7:9]:
        load.wait()
    for first in (HALF, 0):
        turned_queries[pl.ds(first, HALF), :] = rotated(
            rope[pl.ds(first, HALF), :].astype(jnp.float32), first).astype(jnp.bfloat16)
    for load in loads[9:]:
        load.wait()
    pl.semaphore_wait(barrier, 21)

    def query_copies():
        return (
            pltpu.make_async_remote_copy(
                nope.at[pl.ds(HALF, HALF)], far_nope, query_send.at[0], query_recv.at[0],
                device_id=(mirror, t), device_id_type=MESH),
            pltpu.make_async_remote_copy(
                turned_queries.at[pl.ds(HALF, HALF)], far_rope, query_send.at[1], query_recv.at[1],
                device_id=(mirror, t), device_id_type=MESH),
        )

    def piece(kind, block, rows):
        first, count = rows
        if kind == 0:
            return lat.at[4 * block + mine, pl.ds(first // 2, count // 2)]
        return weights_all.at[block, pl.ds(first * 33 // 10, count * 33 // 10)]

    def shard_copy(kind, phase, index):
        source, rows, step, slot = SENDS[phase][index]
        number = sum(len(one) for one in SENDS[:phase]) + index
        place = at_receiver(source, step)
        there = piece(kind, sp_at(*source), rows)
        return pltpu.make_async_remote_copy(
            there, there,
            (send_sem, mixer_send)[kind].at[number], (recv_sem, mixer_recv)[kind].at[4 * place + slot],
            device_id=(sp_at(*step), t), device_id_type=MESH)

    def start_phase(kind, phase):
        for index in range(len(SENDS[phase])):
            shard_copy(kind, phase, index).start()

    def wait_received(kind, phase, first_index=0, last_index=12):
        for source, rows, step, slot in SENDS[phase][first_index:last_index]:
            place = at_receiver(source, step)
            there = piece(kind, sp_at(*ORDER[place]), rows)
            pltpu.make_async_remote_copy(
                there, there,
                (send_sem, mixer_send)[kind].at[0], (recv_sem, mixer_recv)[kind].at[4 * place + slot],
                device_id=(sp_at(*step), t), device_id_type=MESH).wait_recv()

    def pair_copy(place, quarter, number):
        there = lat.at[4 * sp_at(*ORDER[place]) + quarter]
        return pltpu.make_async_remote_copy(
            there, there, pair_send.at[number], pair_recv.at[number],
            device_id=(s, partner), device_id_type=MESH)

    def side_copy(place):
        there = lat.at[4 * sp_at(*ORDER[place]) + mine]
        return pltpu.make_async_remote_copy(
            there, there, side_send.at[place], side_recv.at[place],
            device_id=(s, tp_at(1 - 2 * core)), device_id_type=MESH)

    def hand_on(places):
        for place in places:
            side_copy(place).start()
            pair_copy(place, mine, place).start()

    def side_arrived(place):
        there = lat.at[4 * sp_at(pick(place, [pair[0] for pair in ORDER]), pick(place, [pair[1] for pair in ORDER])) + beside]
        pltpu.make_async_remote_copy(
            there, there, side_send.at[place], side_recv.at[place],
            device_id=(s, partner), device_id_type=MESH).wait_recv()
        pltpu.make_async_remote_copy(
            there, there, pair_send.at[16 + place], pair_recv.at[16 + place],
            device_id=(s, partner), device_id_type=MESH).start()

    def out_copy(number, slot, rows, target):
        first, count = rows
        source = w_out.at[pl.ds(first, count)] if number < 9 else w_out_all.at[slot, pl.ds(first, count)]
        return pltpu.make_async_remote_copy(
            source, w_out_all.at[slot, pl.ds(first, count)],
            out_send.at[number], out_recv.at[number],
            device_id=(s, target), device_id_type=MESH)

    whole, upper, lower = (0, 256), (0, 128), (128, 128)
    right, left, across = tp_at(1), tp_at(3), tp_at(2)
    chunks = tuple((64 * chunk, 64) for chunk in range(4))
    out_sends = (
        *((chunk, t, chunks[chunk], right) for chunk in range(4)),
        *((4 + chunk, t, chunks[chunk], left) for chunk in range(4)),
        (8, t, whole, partner),
        (9, right, upper, left), (10, left, lower, right),
        (11, right, whole, partner), (12, left, whole, partner), (13, across, whole, partner),
    )

    def other(slot):
        return (slot // 2) * 2 + 1 - slot % 2

    out_receives = (
        *((chunk, left, chunks[chunk]) for chunk in range(4)),
        *((4 + chunk, right, chunks[chunk]) for chunk in range(4)),
        (8, partner, whole),
        (9, across, upper), (10, across, lower),
        (11, other(right), whole), (12, other(left), whole), (13, other(across), whole),
    )

    def out_chunk(chunk):
        out_copy(*out_sends[3 - chunk]).start()
        out_copy(*out_sends[4 + chunk]).start()

    def out_wait(number):
        _, slot, (first, count) = out_receives[number]
        pltpu.make_async_remote_copy(
            w_out_all.at[slot, pl.ds(first, count)], w_out_all.at[slot, pl.ds(first, count)],
            out_send.at[number], out_recv.at[number],
            device_id=(s, partner), device_id_type=MESH).wait_recv()

    start_phase(0, 0)
    for copy in query_copies():
        copy.start()
    out_copy(*out_sends[8]).start()
    own_out = pltpu.make_async_copy(w_out, w_out_all.at[t], local_sem.at[1])
    own_out.start()

    w_value_t[...] = jnp.transpose(w_value[...].astype(jnp.float32)).astype(jnp.bfloat16)
    top[...] = jnp.full_like(top, masked_score)
    total[...] = jnp.zeros_like(total)
    acc[...] = jnp.zeros_like(acc)

    lanes = lax.broadcasted_iota(jnp.int32, (HALF, 128), 1)

    def set_queries(group, nope_rows, rope_rows):
        wide = rope_rows.astype(jnp.float32)
        turned = pltpu.roll(wide, 64, 1)
        front = lanes < 64
        for head in range(2):
            one = jnp.transpose(nope_rows[:, head * NOPE:(head + 1) * NOPE].astype(jnp.float32))
            low, high = (wide, turned) if head == 0 else (turned, wide)
            for version, tail in enumerate((jnp.where(front, low, 0.0), jnp.where(front, 0.0, high))):
                queries[group, head, version, 0:NOPE, :] = one.astype(jnp.bfloat16)
                queries[group, head, version, NOPE:2 * NOPE, :] = jnp.transpose(tail).astype(jnp.bfloat16)

    hand_on((0,))
    out_chunk(0)
    set_queries(0, nope[pl.ds(0, HALF), :], turned_queries[pl.ds(0, HALF), :])

    def expand(block):
        for chunk in range(4):
            version, side = chunk // 2, chunk % 2
            quarters = (4 * block + 2 * side, 4 * block + 2 * side + 1)
            rows = jnp.concatenate([lat[one, pl.ds(128 * version, 128), :] for one in quarters], axis=0)
            expanded = jnp.dot(rows, w_key[...], preferred_element_type=jnp.float32).astype(jnp.bfloat16)
            for head in range(2):
                keys[head, pl.ds(256 * chunk, 256), 0:NOPE] = expanded[:, head * NOPE:(head + 1) * NOPE]
                for at in range(4):
                    keys[head, pl.ds(256 * chunk + 64 * at, 64), NOPE:2 * NOPE] = (
                        lat[quarters[at // 2], pl.ds(QUARTER, 64), (at % 2) * 128:(at % 2 + 1) * 128])
            values_t[:, 256 * chunk:256 * (chunk + 1)] = lax.dot_general(
                w_value_t[...], rows, (((1,), (1,)), ((), ())), preferred_element_type=jnp.float32
            ).astype(jnp.bfloat16)

    def fold(group, masked):
        def make(piece_at):
            head, first = piece_at // 2, (piece_at % 2) * 256
            largest = top[group, head, :, first:first + 256]
            for chunk in range(4):
                scores = jnp.dot(
                    keys[head, pl.ds(256 * chunk, 256), :],
                    queries[group, head, chunk // 2, :, first:first + 256],
                    preferred_element_type=jnp.float32)
                if masked:
                    row = lax.broadcasted_iota(jnp.int32, scores.shape, 0)
                    key_at = row + jnp.where(row >= 128, 128, 0) + (512 * (chunk % 2) + 128 * (chunk // 2))
                    query_at = lax.broadcasted_iota(jnp.int32, scores.shape, 1) + (first + HALF * group)
                    scores = jnp.where(key_at <= query_at, scores, masked_score)
                held[piece_at % 2, pl.ds(256 * chunk, 256), :] = scores
                largest = jnp.maximum(largest, jnp.max(scores, axis=0, keepdims=True))
            return largest

        after = make(0)
        for piece_at in range(4):
            following = make(piece_at + 1) if piece_at < 3 else None
            head, first = piece_at // 2, (piece_at % 2) * 256
            columns = slice(first, first + 256)
            before = top[group, head, :, columns]
            offset = after * score_base2
            added = jnp.zeros((1, 256), jnp.float32)
            mixed = jnp.zeros((VDIM, 256), jnp.float32)
            for chunk in range(4):
                weights = jnp.exp2(held[piece_at % 2, pl.ds(256 * chunk, 256), :] * score_base2 - offset)
                added += jnp.sum(weights, axis=0, keepdims=True)
                mixed += jnp.dot(
                    values_t[head * VDIM:(head + 1) * VDIM, 256 * chunk:256 * (chunk + 1)],
                    weights.astype(jnp.bfloat16), preferred_element_type=jnp.float32)
            factor = jnp.exp2((before - after) * score_base2)
            total[group, head, :, columns] = total[group, head, :, columns] * factor + added
            acc[group, head, :, columns] = acc[group, head, :, columns] * factor + mixed
            top[group, head, :, columns] = after
            after = following

    def process(block, place):
        @pl.when(block <= jnp.maximum(s, mirror))
        def _():
            expand(block)

        def one(group, carry):
            last = jnp.where(group == 0, s, mirror)

            @pl.when((place == 0) & (group == 1))
            def _():
                wait_received(0, 0)
                start_phase(0, 1)
                hand_on((1, 2, 3, 4))
                start_phase(1, 0)
                for copy in query_copies():
                    copy.wait_recv()
                set_queries(1, far_nope[...], far_rope[...])

            @pl.when(block < last)
            def _():
                fold(group, False)

            @pl.when(block == last)
            def _():
                fold(group, True)

            return carry

        lax.fori_loop(0, 2, one, 0)

    def advance(place, carry):
        @pl.when(place == 1)
        def _():
            wait_received(0, 1, 0, 4)
            start_phase(0, 2)
            hand_on((5, 6))

        @pl.when(place == 2)
        def _():
            wait_received(0, 1, 4, 12)
            start_phase(0, 3)
            hand_on((7, 8, 9, 10))

        @pl.when(place == 5)
        def _():
            wait_received(0, 2)
            wait_received(0, 3)
            start_phase(0, 4)
            hand_on((11, 12, 13, 14))
            wait_received(1, 0)
            start_phase(1, 1)

        @pl.when(place == 9)
        def _():
            wait_received(0, 4)
            hand_on((15,))
            out_chunk(1)
            out_chunk(2)
            out_chunk(3)

        @pl.when(place == 14)
        def _():
            wait_received(1, 1, 0, 4)
            start_phase(1, 2)

        @pl.when(place <= 1)
        def _():
            side_arrived(place)

        @pl.when((place >= 1) & (place < 15))
        def _():
            side_arrived(place + 1)

        dy = pick(place, [pair[0] for pair in ORDER])
        dz = pick(place, [pair[1] for pair in ORDER])
        block = sp_at(dy, dz)
        for number, quarter in ((place, 2 * (x % 2) + 1 - core), (16 + place, 2 * (1 - x % 2) + 1 - core)):
            theirs = lat.at[4 * block + quarter]
            pltpu.make_async_remote_copy(
                theirs, theirs, pair_send.at[number], pair_recv.at[number],
                device_id=(s, partner), device_id_type=MESH).wait_recv()
        process(block, place)
        return carry

    lax.fori_loop(0, 16, advance, 0)

    for group in range(2):
        for head in range(2):
            mixed = acc[group, head] / total[group, head]
            head_out[group, :, head * VDIM:(head + 1) * VDIM] = jnp.transpose(mixed).astype(jnp.bfloat16)

    def head_copy(group, part):
        target = part if group == 0 else 4 + part
        return pltpu.make_async_remote_copy(
            head_out.at[group, pl.ds(128 * part, 128)], heads_all.at[t],
            head_send.at[4 * group + part], head_recv.at[t],
            device_id=(s if group == 0 else mirror, target), device_id_type=MESH)

    for part in range(4):
        head_copy(1, part).start()

        @pl.when(t != part)
        def _():
            head_copy(0, part).start()

    @pl.when(t < 4)
    def _():
        mine = pltpu.make_async_copy(
            head_out.at[0, pl.ds(128 * (t % 4), 128)], heads_all.at[t], local_sem.at[2])
        mine.start()
        mine.wait()

    for number in (2, 3, 4, 5):
        out_wait(number)
    for number in (9, 10):
        out_copy(*out_sends[number]).start()
    wait_received(1, 1, 4, 12)
    start_phase(1, 3)

    def head_wait(slot, carry):
        @pl.when((t >= 4) | (slot != t))
        def _():
            pltpu.make_async_remote_copy(
                head_out.at[0, pl.ds(0, 128)], heads_all.at[slot], head_send.at[0], head_recv.at[slot],
                device_id=(mirror, t), device_id_type=MESH).wait_recv()

        return carry

    own_out.wait()
    for number in (0, 1, 6, 7):
        out_wait(number)
    for number in (11, 12):
        out_copy(*out_sends[number]).start()
    lax.fori_loop(0, 8, head_wait, 0)
    wait_received(1, 2)
    wait_received(1, 3)
    start_phase(1, 4)
    for number in (8, 11, 12):
        out_wait(number)

    stream[...] = resid[...].astype(jnp.float32)

    def project(turn, carry):
        @pl.when(turn == 6)
        def _():
            for number in (9, 10):
                out_wait(number)
            out_copy(*out_sends[13]).start()

        @pl.when(turn == 7)
        def _():
            out_wait(13)

        slot = pick(turn, (0, 1, 2, 3, 6, 7, 4, 5))
        slot = (2 * x + core + slot - 2 * ((core + slot % 2) // 2)) % 8
        stream[...] += jnp.dot(heads_all[slot], w_out_all[slot], preferred_element_type=jnp.float32)
        return carry

    lax.fori_loop(0, 8, project, 0)
    rows_f32 = stream[...]
    scale = lax.rsqrt(jnp.mean(rows_f32 * rows_f32, axis=-1, keepdims=True) + norm_eps)
    rows_all[t] = (rows_f32 * scale * mix_gain[...]).astype(jnp.bfloat16)

    high, low = (0, 64), (64, 64)
    all_rows = (0, 128)
    row_sends = (
        (0, t, all_rows, right), (1, t, all_rows, left), (2, t, all_rows, partner),
        (3, right, high, left), (4, left, low, right),
        (5, right, all_rows, partner), (6, left, all_rows, partner), (7, across, all_rows, partner),
    )
    row_receives = (
        (0, left, all_rows), (1, right, all_rows), (2, partner, all_rows),
        (3, across, high), (4, across, low),
        (5, other(right), all_rows), (6, other(left), all_rows), (7, other(across), all_rows),
    )

    def row_copy(number):
        _, slot, (first, count), target = row_sends[number]
        here = rows_all.at[slot, pl.ds(first, count)]
        return pltpu.make_async_remote_copy(
            here, here, row_send.at[number], row_recv.at[number],
            device_id=(s, target), device_id_type=MESH)

    def row_wait(number):
        _, slot, (first, count) = row_receives[number]
        here = rows_all.at[slot, pl.ds(first, count)]
        pltpu.make_async_remote_copy(
            here, here, row_send.at[number], row_recv.at[number],
            device_id=(s, partner), device_id_type=MESH).wait_recv()

    for number in range(3):
        row_copy(number).start()

    wait_received(1, 4)

    def part_copy(step):
        return pltpu.make_async_remote_copy(
            halves.at[step, 1 - core], got.at[step], part_send.at[step], part_recv.at[step],
            device_id=(s, partner), device_id_type=MESH)

    def chip_total(step):
        part_copy(step).wait_recv()
        return halves[step, core].astype(jnp.float32) + got[step].astype(jnp.float32)

    def sum_copy(number):
        here, there, target = (
            (summed.at[1], arrived.at[0], right),
            (summed.at[2], arrived.at[1], left),
            (summed.at[3, pl.ds(0, 64)], relay.at[0], right),
            (summed.at[3, pl.ds(64, 64)], relay.at[1], left),
            (relay.at[0], arrived.at[2, pl.ds(0, 64)], right),
            (relay.at[1], arrived.at[2, pl.ds(64, 64)], left),
        )[number]
        return pltpu.make_async_remote_copy(
            here, there, sum_send.at[number], sum_recv.at[number],
            device_id=(s, target), device_id_type=MESH)

    def mix(step, carry):
        @pl.when(step == 0)
        def _():
            row_wait(2)

        @pl.when(step == 1)
        def _():
            row_wait(0)
            row_wait(1)
            for number in (3, 4, 5, 6):
                row_copy(number).start()
            row_wait(5)
            row_wait(6)

        @pl.when(step == 2)
        def _():
            row_wait(3)
            row_wait(4)
            row_copy(7).start()

        @pl.when(step == 3)
        def _():
            row_wait(7)

        chip = (x + pick(step, (0, 1, 3, 2))) % SIDE

        def columns(pair, first, count):
            return jnp.concatenate([weights_all[2 * pair + side, pl.ds(first, count), :] for side in range(2)], axis=1)

        def product(first, count):
            added = jnp.zeros((256, count), jnp.float32)
            for pair in range(8):
                rows = rows_all[pl.ds(2 * chip, 2), :, 256 * pair:256 * (pair + 1)].reshape(256, 256)
                added += lax.dot_general(
                    rows, columns(pair, first, count), (((1,), (1,)), ((), ())), preferred_element_type=jnp.float32)
            return added

        for first, count in ((0, 256), (256, 256), (512, 192)):
            gate_value, upward = product(first, count), product(UNITS + first, count)
            hidden[:, first:first + count] = (gate_value / (1.0 + jnp.exp(-gate_value)) * upward).astype(jnp.bfloat16)
        for pair in range(8):
            down = jnp.dot(hidden[...], columns(pair, 2 * UNITS, UNITS), preferred_element_type=jnp.float32)
            halves[step, :, :, 256 * pair:256 * (pair + 1)] = down.astype(jnp.bfloat16).reshape(2, 128, 256)
        part_copy(step).start()

        @pl.when(step == 1)
        def _():
            stream[...] += 0.5 * chip_total(0)

        @pl.when(step == 2)
        def _():
            summed[1] = chip_total(1).astype(jnp.bfloat16)
            sum_copy(0).start()

        @pl.when(step == 3)
        def _():
            summed[2] = chip_total(2).astype(jnp.bfloat16)
            sum_copy(1).start()

        return carry

    lax.fori_loop(0, 4, mix, 0)
    summed[3] = chip_total(3).astype(jnp.bfloat16)
    sum_copy(2).start()
    sum_copy(3).start()
    sum_copy(2).wait_recv()
    sum_copy(4).start()
    sum_copy(3).wait_recv()
    sum_copy(5).start()
    sum_copy(0).wait_recv()
    sum_copy(1).wait_recv()
    stream[...] += 0.5 * (arrived[0].astype(jnp.float32) + arrived[1].astype(jnp.float32))
    sum_copy(4).wait_recv()
    sum_copy(5).wait_recv()
    result[...] = (stream[...] + 0.5 * arrived[2].astype(jnp.float32)).astype(jnp.bfloat16)

    for number in range(6):
        sum_copy(number).wait_send()
    for step in range(4):
        part_copy(step).wait_send()
    for number in range(8):
        row_copy(number).wait_send()
    for number in range(14):
        out_copy(*out_sends[number]).wait_send()
    for copy in query_copies():
        copy.wait_send()
    for phase in range(len(SENDS)):
        for index in range(len(SENDS[phase])):
            shard_copy(0, phase, index).wait_send()
            shard_copy(1, phase, index).wait_send()
    for place in range(16):
        side_copy(place).wait_send()
        pair_copy(place, mine, place).wait_send()
        pair_copy(place, beside, 16 + place).wait_send()
    for number in range(4):
        head_copy(1, number).wait_send()

        @pl.when(t != number)
        def _():
            head_copy(0, number).wait_send()


def layer_call(*operands):
    vmem = pl.BlockSpec(memory_space=pltpu.VMEM)
    anywhere = pl.BlockSpec(memory_space=pl.ANY)
    dma = pltpu.SemaphoreType.DMA
    bf16, f32 = jnp.bfloat16, jnp.float32
    return pl.pallas_call(
        layer_kernel,
        out_shape=jax.ShapeDtypeStruct((128, 2048), bf16),
        in_specs=[anywhere] * len(operands),
        out_specs=vmem,
        scratch_shapes=[
            pltpu.VMEM((ROWS, 256), bf16),
            pltpu.VMEM((ROWS, 128), bf16),
            pltpu.VMEM((QUARTER, 256), bf16),
            pltpu.VMEM((ROPE, QUARTER), bf16),
            pltpu.VMEM((1, 256), f32),
            pltpu.VMEM((256, 256), bf16),
            pltpu.VMEM((256, 256), bf16),
            pltpu.VMEM((128, 2048), bf16),
            pltpu.VMEM((1, 2048), f32),
            pltpu.VMEM((ROWS, 128), f32),
            pltpu.VMEM((ROWS, 128), f32),
            pltpu.VMEM((16, 128), f32),
            pltpu.VMEM((16, 128), f32),
            pltpu.VMEM((ROWS, 128), bf16),
            pltpu.VMEM((64, SHARD, 256), bf16),
            pltpu.VMEM((HALF, 256), bf16),
            pltpu.VMEM((HALF, 128), bf16),
            pltpu.VMEM((2, 2, 2, 256, HALF), bf16),
            pltpu.VMEM((2, ROWS, 256), bf16),
            pltpu.VMEM((256, ROWS), bf16),
            pltpu.VMEM((2, ROWS, 256), f32),
            pltpu.VMEM((256, 256), bf16),
            pltpu.VMEM((2, 2, 1, HALF), f32),
            pltpu.VMEM((2, 2, 1, HALF), f32),
            pltpu.VMEM((2, 2, VDIM, HALF), f32),
            pltpu.VMEM((2, HALF, 256), bf16),
            pltpu.VMEM((8, 128, 256), bf16),
            pltpu.VMEM((8, 256, 2048), bf16),
            pltpu.VMEM((16, 3 * UNITS, 128), bf16),
            pltpu.VMEM((256, UNITS), bf16),
            pltpu.VMEM((128, 2048), f32),
            pltpu.VMEM((8, 128, 2048), bf16),
            pltpu.VMEM((4, 2, 128, 2048), bf16),
            pltpu.VMEM((4, 128, 2048), bf16),
            pltpu.VMEM((4, 128, 2048), bf16),
            pltpu.VMEM((2, 64, 2048), bf16),
            pltpu.VMEM((3, 128, 2048), bf16),
            dma((32,)), dma((64,)), dma((16,)), dma((16,)), dma((32,)), dma((32,)), dma((2,)), dma((2,)),
            dma((8,)), dma((8,)), dma((14,)), dma((14,)), dma((4,)),
            dma((32,)), dma((64,)), dma((8,)), dma((8,)), dma((4,)), dma((4,)), dma((6,)), dma((6,)), dma((16,)),
        ],
        compiler_params=pltpu.CompilerParams(
            collective_id=0, has_side_effects=True, vmem_limit_bytes=67_000_000),
        cost_estimate=pl.CostEstimate(flops=60_000_000_000, bytes_accessed=30_000_000, transcendentals=18_000_000),
        name="layer",
    )(*operands)


def angle_tables(positions):
    frequency = theta_base ** (-2.0 * np.arange(ROPE // 2) / ROPE)
    angle = np.tile(np.asarray(positions, np.float64)[:, None] * frequency[None, :], (1, 4))
    return np.cos(angle).astype(np.float32), np.sin(angle).astype(np.float32)


def on_device(
    resid, query_nope, query_rope, latent, key_rope, latent_gain, w_key, w_value, w_out, mix_gain,
    w_gate, w_up, w_down,
):
    row_tables = angle_tables(np.arange(ROWS))
    block_tables = angle_tables(ROWS * np.arange(16))
    return layer_call(
        query_nope, query_rope, latent, key_rope.T, latent_gain.reshape(1, -1), w_key, w_value, w_out, resid,
        mix_gain.reshape(1, -1), w_gate.T, w_up.T, w_down.T,
        *(jnp.asarray(table) for table in row_tables + block_tables))


def solution(mesh):
    return jax.shard_map(
        on_device,
        mesh=mesh,
        in_specs=(
            P(("sp", "tp"), None),
            P("sp", "tp"),
            P("sp", "tp"),
            P("sp", None),
            P("sp", None),
            P(),
            P(None, "tp"),
            P(None, "tp"),
            P("tp", None),
            P(),
            P("sp", "tp"),
            P("sp", "tp"),
            P("sp", "tp"),
        ),
        out_specs=P(("sp", "tp"), None),
        check_vma=False,
    )
```

```python
import functools

import jax
import jax.numpy as jnp
import numpy as np
from jax import lax
from jax.experimental import pallas as pl
from jax.experimental.pallas import tpu as pltpu
from jax.sharding import PartitionSpec as P

NOPE = 128
ROPE = 64
VDIM = 128
ROWS = 1024
HALF = 512
SIDE = 4
UNITS = 704
SHARD = HALF + HALF // 4

norm_eps = 1e-06
masked_score = -1e30
theta_base = 10000.0
score_base2 = (NOPE + ROPE) ** (-0.5) * 1.4426950408889634
MESH = pl.DeviceIdType.MESH

ORDER = ((0, 0), (1, 0), (3, 0), (0, 1), (0, 3), (2, 0), (0, 2), (1, 1), (1, 3), (3, 1), (3, 3),
         (2, 1), (2, 3), (1, 2), (3, 2), (2, 2))
PLACE = {pair: p for p, pair in enumerate(ORDER)}
ALPHA, BETA, FULL = (0, 320), (320, 320), (0, 640)
ALPHA0, ALPHA1, BETA0, BETA1 = (0, 160), (160, 160), (320, 160), (480, 160)

SENDS = (
    (((0, 0), FULL, (1, 0), 0), ((0, 0), FULL, (-1, 0), 0), ((0, 0), FULL, (0, 1), 0), ((0, 0), FULL, (0, -1), 0)),
    (
        ((1, 0), ALPHA, (-1, 0), 0), ((3, 0), BETA, (1, 0), 1),
        ((0, 1), ALPHA, (0, -1), 0), ((0, 3), BETA, (0, 1), 1),
        ((1, 0), ALPHA, (0, 1), 0), ((1, 0), ALPHA, (0, -1), 0),
        ((3, 0), ALPHA, (0, 1), 0), ((3, 0), ALPHA, (0, -1), 0),
        ((0, 1), BETA, (1, 0), 1), ((0, 1), BETA, (-1, 0), 1),
        ((0, 3), BETA, (1, 0), 1), ((0, 3), BETA, (-1, 0), 1),
    ),
    (
        ((2, 0), ALPHA, (0, 1), 0), ((2, 0), ALPHA, (0, -1), 0),
        ((0, 2), BETA, (1, 0), 1), ((0, 2), BETA, (-1, 0), 1),
    ),
    (
        ((1, 1), ALPHA0, (0, -1), 0), ((1, 3), ALPHA1, (0, 1), 2),
        ((3, 1), ALPHA0, (0, -1), 0), ((3, 3), ALPHA1, (0, 1), 2),
        ((1, 1), BETA0, (-1, 0), 1), ((3, 1), BETA1, (1, 0), 2),
        ((1, 3), BETA0, (-1, 0), 1), ((3, 3), BETA1, (1, 0), 2),
    ),
    (
        ((2, 1), ALPHA0, (0, -1), 0), ((2, 3), ALPHA1, (0, 1), 1),
        ((1, 2), BETA0, (-1, 0), 2), ((3, 2), BETA1, (1, 0), 3),
    ),
)


def at_receiver(source, step):
    return PLACE[((source[0] - step[0]) % SIDE, (source[1] - step[1]) % SIDE)]


def pick(index, values):
    found = jnp.int32(values[0])
    for at in range(1, len(values)):
        found = jnp.where(index == at, jnp.int32(values[at]), found)
    return found


def layer_kernel(
    nope_in, rope_in, latent_in, key_in, gain_in, w_key_in, w_value_in, w_out, resid_in, mix_gain_in,
    gate_in, up_in, down_in, row_cos_in, row_sin_in, block_cos_in, block_sin_in, result,
    nope, rope, latent, key_rope, gain, w_key, w_value, resid, mix_gain,
    row_cos, row_sin, block_cos, block_sin, turned_queries,
    lat, far_nope, far_rope, queries, keys, values_t, held, w_value_t, top, total, acc, head_out,
    heads_all, w_out_all, weights_all, hidden, stream, rows_all, halves, got, summed, relay, arrived, waiting,
    send_sem, recv_sem, pair_send, pair_recv, query_send, query_recv, head_send, head_recv,
    out_send, out_recv, local_sem, mixer_send, mixer_recv, row_send, row_recv, part_send, part_recv,
    sum_send, sum_recv, load_sem,
):
    s = lax.axis_index("sp")
    t = lax.axis_index("tp")
    z, y = s // SIDE, s % SIDE
    x, core = t // 2, t % 2
    mirror = 15 - s

    def sp_at(dy, dz):
        return ((z + dz + SIDE) % SIDE) * SIDE + (y + dy + SIDE) % SIDE

    def tp_at(dx):
        return ((x + dx + SIDE) % SIDE) * 2 + core

    partner = x * 2 + 1 - core

    barrier = pltpu.get_barrier_semaphore()
    for step in (1, 2, 3):
        pl.semaphore_signal(barrier, inc=1, device_id=(sp_at(step, 0), t), device_id_type=MESH)
        pl.semaphore_signal(barrier, inc=1, device_id=(sp_at(0, step), t), device_id_type=MESH)
    for step in range(1, 8):
        pl.semaphore_signal(barrier, inc=1, device_id=(s, (t + step) % 8), device_id_type=MESH)
    for step in range(8):
        pl.semaphore_signal(barrier, inc=1, device_id=(mirror, (t + step) % 8), device_id_type=MESH)

    half_rows = pl.ds(pl.multiple_of(core * HALF, HALF), HALF)
    loads = [
        pltpu.make_async_copy(source, target, load_sem.at[number])
        for number, (source, target) in enumerate((
            (latent_in.at[half_rows], latent), (key_in.at[:, half_rows], key_rope), (gain_in, gain),
            (block_cos_in, block_cos), (block_sin_in, block_sin), (row_cos_in, row_cos), (row_sin_in, row_sin),
            (rope_in, rope), (nope_in, nope), (w_value_in, w_value), (w_key_in, w_key),
            (gate_in, weights_all.at[s, pl.ds(0, UNITS)]), (up_in, weights_all.at[s, pl.ds(UNITS, UNITS)]),
            (down_in, weights_all.at[s, pl.ds(2 * UNITS, UNITS)]), (resid_in, resid), (mix_gain_in, mix_gain),
        ))
    ]
    for load in loads:
        load.start()

    def rotated(rows_in, first):
        count = rows_in.shape[0]
        at = pl.ds(first, count)
        near_cos, near_sin = row_cos[at, :], row_sin[at, :]
        far_cos, far_sin = block_cos[pl.ds(s, 1), :], block_sin[pl.ds(s, 1), :]
        cosine = far_cos * near_cos - far_sin * near_sin
        sine = far_sin * near_cos + far_cos * near_sin
        lane = lax.broadcasted_iota(jnp.int32, rows_in.shape, 1) % ROPE
        swapped = jnp.where(lane < ROPE // 2, -pltpu.roll(rows_in, 96, 1), pltpu.roll(rows_in, 32, 1))
        return rows_in * cosine + swapped * sine

    own = 2 * s + core
    for load in loads[:7]:
        load.wait()
    wide = latent[...].astype(jnp.float32)
    scale = lax.rsqrt(jnp.mean(wide * wide, axis=-1, keepdims=True) + norm_eps)
    lat[own, pl.ds(0, HALF), :] = (wide * scale * gain[...]).astype(jnp.bfloat16)
    once = key_rope[...].astype(jnp.float32)
    twice = rotated(jnp.transpose(jnp.concatenate([once, once], axis=0)), core * HALF).astype(jnp.bfloat16)
    front_lanes = lax.broadcasted_iota(jnp.int32, (128, 128), 1) < ROPE
    for side in range(2):
        lat[own, pl.ds(HALF, 128), side * 128:(side + 1) * 128] = jnp.where(
            front_lanes, twice[128 * side:128 * side + 128], twice[256 + 128 * side:384 + 128 * side])
    for load in loads[7:9]:
        load.wait()
    for first in (HALF, 0):
        turned_queries[pl.ds(first, HALF), :] = rotated(
            rope[pl.ds(first, HALF), :].astype(jnp.float32), first).astype(jnp.bfloat16)
    for load in loads[9:]:
        load.wait()
    pl.semaphore_wait(barrier, 21)

    def query_copies():
        return (
            pltpu.make_async_remote_copy(
                nope.at[pl.ds(HALF, HALF)], far_nope, query_send.at[0], query_recv.at[0],
                device_id=(mirror, t), device_id_type=MESH),
            pltpu.make_async_remote_copy(
                turned_queries.at[pl.ds(HALF, HALF)], far_rope, query_send.at[1], query_recv.at[1],
                device_id=(mirror, t), device_id_type=MESH),
        )

    def piece(kind, block, rows):
        first, count = rows
        if kind == 0:
            return lat.at[2 * block + core, pl.ds(first, count)]
        return weights_all.at[block, pl.ds(first * 33 // 10, count * 33 // 10)]

    def shard_copy(kind, phase, index):
        source, rows, step, slot = SENDS[phase][index]
        number = sum(len(one) for one in SENDS[:phase]) + index
        place = at_receiver(source, step)
        there = piece(kind, sp_at(*source), rows)
        return pltpu.make_async_remote_copy(
            there, there,
            (send_sem, mixer_send)[kind].at[number], (recv_sem, mixer_recv)[kind].at[4 * place + slot],
            device_id=(sp_at(*step), t), device_id_type=MESH)

    def start_phase(kind, phase, first_index=0, last_index=12):
        for index in range(len(SENDS[phase]))[first_index:last_index]:
            shard_copy(kind, phase, index).start()

    def wait_received(kind, phase, first_index=0, last_index=12):
        for source, rows, step, slot in SENDS[phase][first_index:last_index]:
            place = at_receiver(source, step)
            there = piece(kind, sp_at(*ORDER[place]), rows)
            pltpu.make_async_remote_copy(
                there, there,
                (send_sem, mixer_send)[kind].at[0], (recv_sem, mixer_recv)[kind].at[4 * place + slot],
                device_id=(sp_at(*step), t), device_id_type=MESH).wait_recv()

    def pair_copy(place):
        there = lat.at[2 * sp_at(*ORDER[place]) + core]
        return pltpu.make_async_remote_copy(
            there, there, pair_send.at[place], pair_recv.at[place],
            device_id=(s, partner), device_id_type=MESH)

    def hand_on(places):
        for place in places:
            pair_copy(place).start()

    def out_copy(number, slot, rows, target):
        first, count = rows
        source = w_out.at[pl.ds(first, count)] if number < 9 else w_out_all.at[slot, pl.ds(first, count)]
        return pltpu.make_async_remote_copy(
            source, w_out_all.at[slot, pl.ds(first, count)],
            out_send.at[number], out_recv.at[number],
            device_id=(s, target), device_id_type=MESH)

    whole, upper, lower = (0, 256), (0, 128), (128, 128)
    right, left, across = tp_at(1), tp_at(3), tp_at(2)
    chunks = tuple((64 * chunk, 64) for chunk in range(4))
    out_sends = (
        *((chunk, t, chunks[chunk], right) for chunk in range(4)),
        *((4 + chunk, t, chunks[chunk], left) for chunk in range(4)),
        (8, t, whole, partner),
        (9, right, upper, left), (10, left, lower, right),
        (11, right, whole, partner), (12, left, whole, partner), (13, across, whole, partner),
    )

    def other(slot):
        return (slot // 2) * 2 + 1 - slot % 2

    out_receives = (
        *((chunk, left, chunks[chunk]) for chunk in range(4)),
        *((4 + chunk, right, chunks[chunk]) for chunk in range(4)),
        (8, partner, whole),
        (9, across, upper), (10, across, lower),
        (11, other(right), whole), (12, other(left), whole), (13, other(across), whole),
    )

    def out_chunk(chunk):
        out_copy(*out_sends[3 - chunk]).start()
        out_copy(*out_sends[4 + chunk]).start()

    def out_wait(number):
        _, slot, (first, count) = out_receives[number]
        pltpu.make_async_remote_copy(
            w_out_all.at[slot, pl.ds(first, count)], w_out_all.at[slot, pl.ds(first, count)],
            out_send.at[number], out_recv.at[number],
            device_id=(s, partner), device_id_type=MESH).wait_recv()

    start_phase(0, 0)
    for copy in query_copies():
        copy.start()
    out_copy(*out_sends[8]).start()
    own_out = pltpu.make_async_copy(w_out, w_out_all.at[t], local_sem.at[1])
    own_out.start()

    w_value_t[...] = jnp.transpose(w_value[...].astype(jnp.float32)).astype(jnp.bfloat16)
    top[...] = jnp.full_like(top, masked_score)
    total[...] = jnp.zeros_like(total)
    acc[...] = jnp.zeros_like(acc)

    lanes = lax.broadcasted_iota(jnp.int32, (HALF, 128), 1)

    def set_queries(group, nope_rows, rope_rows):
        wide = rope_rows.astype(jnp.float32)
        turned = pltpu.roll(wide, 64, 1)
        front = lanes < 64
        for head in range(2):
            one = jnp.transpose(nope_rows[:, head * NOPE:(head + 1) * NOPE].astype(jnp.float32))
            low, high = (wide, turned) if head == 0 else (turned, wide)
            for version, tail in enumerate((jnp.where(front, low, 0.0), jnp.where(front, 0.0, high))):
                queries[group, head, version, 0:NOPE, :] = one.astype(jnp.bfloat16)
                queries[group, head, version, NOPE:2 * NOPE, :] = jnp.transpose(tail).astype(jnp.bfloat16)

    hand_on((0,))
    for chunk in range(4):
        out_chunk(chunk)
    set_queries(0, nope[pl.ds(0, HALF), :], turned_queries[pl.ds(0, HALF), :])

    def expand(block):
        for plane in range(2):
            rows = lat[2 * block + plane, pl.ds(0, HALF), :]
            expanded = jnp.dot(rows, w_key[...], preferred_element_type=jnp.float32).astype(jnp.bfloat16)
            tails = tuple(lat[2 * block + plane, pl.ds(HALF, 128), side * 128:(side + 1) * 128] for side in range(2))
            for head in range(2):
                keys[head, pl.ds(plane * HALF, HALF), 0:NOPE] = expanded[:, head * NOPE:(head + 1) * NOPE]
                for quarter in range(4):
                    keys[head, pl.ds(plane * HALF + quarter * 128, 128), NOPE:2 * NOPE] = tails[quarter % 2]
            values_t[:, plane * HALF:(plane + 1) * HALF] = lax.dot_general(
                w_value_t[...], rows, (((1,), (1,)), ((), ())), preferred_element_type=jnp.float32
            ).astype(jnp.bfloat16)

    def fold(group, masked):
        def make(piece_at):
            head, first = piece_at // 2, (piece_at % 2) * 256
            largest = top[group, head, :, first:first + 256]
            for chunk in range(4):
                scores = jnp.dot(
                    keys[head, pl.ds(256 * chunk, 256), :],
                    queries[group, head, chunk % 2, :, first:first + 256],
                    preferred_element_type=jnp.float32)
                if masked:
                    key_at = lax.broadcasted_iota(jnp.int32, scores.shape, 0) + 256 * chunk
                    query_at = lax.broadcasted_iota(jnp.int32, scores.shape, 1) + (first + HALF * group)
                    scores = jnp.where(key_at <= query_at, scores, masked_score)
                held[piece_at % 2, pl.ds(256 * chunk, 256), :] = scores
                largest = jnp.maximum(largest, jnp.max(scores, axis=0, keepdims=True))
            return largest

        after = make(0)
        for piece_at in range(4):
            following = make(piece_at + 1) if piece_at < 3 else None
            head, first = piece_at // 2, (piece_at % 2) * 256
            columns = slice(first, first + 256)
            before = top[group, head, :, columns]
            offset = after * score_base2
            added = jnp.zeros((1, 256), jnp.float32)
            mixed = jnp.zeros((VDIM, 256), jnp.float32)
            for chunk in range(4):
                weights = jnp.exp2(held[piece_at % 2, pl.ds(256 * chunk, 256), :] * score_base2 - offset)
                added += jnp.sum(weights, axis=0, keepdims=True)
                mixed += jnp.dot(
                    values_t[head * VDIM:(head + 1) * VDIM, 256 * chunk:256 * (chunk + 1)],
                    weights.astype(jnp.bfloat16), preferred_element_type=jnp.float32)
            factor = jnp.exp2((before - after) * score_base2)
            total[group, head, :, columns] = total[group, head, :, columns] * factor + added
            acc[group, head, :, columns] = acc[group, head, :, columns] * factor + mixed
            top[group, head, :, columns] = after
            after = following

    def process(block, place):
        @pl.when(block <= jnp.maximum(s, mirror))
        def _():
            expand(block)

        def one(group, carry):
            last = jnp.where(group == 0, s, mirror)

            @pl.when((place == 0) & (group == 1))
            def _():
                wait_received(0, 0)
                start_phase(0, 1)
                hand_on((1, 2, 3, 4))
                for copy in query_copies():
                    copy.wait_recv()
                set_queries(1, far_nope[...], far_rope[...])

            @pl.when(block < last)
            def _():
                fold(group, False)

            @pl.when(block == last)
            def _():
                fold(group, True)

            return carry

        lax.fori_loop(0, 2, one, 0)

    def advance(place, carry):
        @pl.when(place == 1)
        def _():
            wait_received(0, 1, 0, 4)
            start_phase(0, 2)
            hand_on((5, 6))

        @pl.when(place == 3)
        def _():
            wait_received(0, 1, 4, 12)
            start_phase(0, 3)
            hand_on((7, 8, 9, 10))
            start_phase(1, 0)

        @pl.when(place == 6)
        def _():
            wait_received(0, 2)
            wait_received(0, 3)
            start_phase(0, 4)
            hand_on((11, 12, 13, 14))
            for number in (2, 3, 4, 5):
                out_wait(number)
            for number in (9, 10):
                out_copy(*out_sends[number]).start()

        @pl.when(place == 10)
        def _():
            wait_received(1, 0)
            start_phase(1, 1, 0, 4)
            for number in (0, 1, 6, 7):
                out_wait(number)
            for number in (11, 12):
                out_copy(*out_sends[number]).start()

        @pl.when(place == 13)
        def _():
            wait_received(0, 4)
            hand_on((15,))
            for number in (9, 10):
                out_wait(number)
            out_copy(*out_sends[13]).start()
            start_phase(1, 1, 4, 6)
            start_phase(1, 1, 8, 10)

        dy = pick(place, [pair[0] for pair in ORDER])
        dz = pick(place, [pair[1] for pair in ORDER])
        block = sp_at(dy, dz)
        theirs = lat.at[2 * block + 1 - core]
        pltpu.make_async_remote_copy(
            theirs, theirs, pair_send.at[place], pair_recv.at[place],
            device_id=(s, partner), device_id_type=MESH).wait_recv()
        process(block, place)
        return carry

    lax.fori_loop(0, 16, advance, 0)

    def head_copy(group, part):
        target = part if group == 0 else 4 + part
        return pltpu.make_async_remote_copy(
            head_out.at[group, pl.ds(128 * part, 128)], heads_all.at[t],
            head_send.at[4 * group + part], head_recv.at[t],
            device_id=(s if group == 0 else mirror, target), device_id_type=MESH)

    def close(group):
        for head in range(2):
            mixed = acc[group, head] / total[group, head]
            head_out[group, :, head * VDIM:(head + 1) * VDIM] = jnp.transpose(mixed).astype(jnp.bfloat16)

    close(1)
    for number in range(4):
        head_copy(1, number).start()
    close(0)
    for number in range(4):
        @pl.when(t != number)
        def _():
            head_copy(0, number).start()

    @pl.when(t < 4)
    def _():
        mine = pltpu.make_async_copy(
            head_out.at[0, pl.ds(128 * (t % 4), 128)], heads_all.at[t], local_sem.at[2])
        mine.start()
        mine.wait()

    def head_wait(slot, carry):
        @pl.when((t >= 4) | (slot != t))
        def _():
            pltpu.make_async_remote_copy(
                head_out.at[0, pl.ds(0, 128)], heads_all.at[slot], head_send.at[0], head_recv.at[slot],
                device_id=(mirror, t), device_id_type=MESH).wait_recv()

        return carry

    start_phase(1, 1, 6, 8)
    start_phase(1, 1, 10, 12)
    wait_received(1, 1, 0, 4)
    start_phase(1, 2)
    for number in (8, 11, 12, 13):
        out_wait(number)
    own_out.wait()
    lax.fori_loop(0, 8, head_wait, 0)

    stream[...] = resid[...].astype(jnp.float32)

    def project(turn, carry):
        slot = pick(turn, (0, 1, 2, 3, 6, 7, 4, 5))
        slot = (2 * x + core + slot - 2 * ((core + slot % 2) // 2)) % 8
        stream[...] += jnp.dot(heads_all[slot], w_out_all[slot], preferred_element_type=jnp.float32)
        return carry

    lax.fori_loop(0, 8, project, 0)
    rows_f32 = stream[...]
    scale = lax.rsqrt(jnp.mean(rows_f32 * rows_f32, axis=-1, keepdims=True) + norm_eps)
    rows_all[t] = (rows_f32 * scale * mix_gain[...]).astype(jnp.bfloat16)

    high, low = (0, 64), (64, 64)
    all_rows = (0, 128)
    row_sends = (
        (0, t, low, right), (1, t, high, left), (2, t, all_rows, partner),
        (3, right, high, left), (4, left, low, right),
        (5, right, all_rows, partner), (6, left, all_rows, partner), (7, across, all_rows, partner),
        (8, t, high, right), (9, t, low, left),
    )
    row_receives = (
        (0, left, low), (1, right, high), (2, partner, all_rows),
        (3, across, high), (4, across, low),
        (5, other(right), all_rows), (6, other(left), all_rows), (7, other(across), all_rows),
        (8, left, high), (9, right, low),
    )

    def row_copy(number):
        _, slot, (first, count), target = row_sends[number]
        here = rows_all.at[slot, pl.ds(first, count)]
        return pltpu.make_async_remote_copy(
            here, here, row_send.at[number], row_recv.at[number],
            device_id=(s, target), device_id_type=MESH)

    def row_wait(number):
        _, slot, (first, count) = row_receives[number]
        here = rows_all.at[slot, pl.ds(first, count)]
        pltpu.make_async_remote_copy(
            here, here, row_send.at[number], row_recv.at[number],
            device_id=(s, partner), device_id_type=MESH).wait_recv()

    for number in range(3):
        row_copy(number).start()
    row_wait(0)
    row_wait(1)
    for number in (3, 4, 8, 9):
        row_copy(number).start()
    wait_received(1, 1, 4, 12)
    start_phase(1, 3)
    row_wait(2)
    row_wait(3)
    row_wait(4)
    row_copy(7).start()
    wait_received(1, 2)
    wait_received(1, 3)
    start_phase(1, 4)
    row_wait(8)
    row_wait(9)
    row_copy(5).start()
    row_copy(6).start()
    row_wait(7)
    wait_received(1, 4)

    def part_copy(step):
        return pltpu.make_async_remote_copy(
            halves.at[step, 1 - core], got.at[step], part_send.at[step], part_recv.at[step],
            device_id=(s, partner), device_id_type=MESH)

    def chip_total(step):
        part_copy(step).wait_recv()
        return halves[step, core].astype(jnp.float32) + got[step].astype(jnp.float32)

    def sum_copy(number):
        here, there, target = (
            (summed.at[0, pl.ds(0, 64)], relay.at[0], right),
            (summed.at[0, pl.ds(64, 64)], relay.at[1], left),
            (summed.at[1, pl.ds(64, 64)], arrived.at[0, pl.ds(64, 64)], right),
            (summed.at[2, pl.ds(0, 64)], arrived.at[1, pl.ds(0, 64)], left),
            (summed.at[1, pl.ds(0, 64)], arrived.at[0, pl.ds(0, 64)], right),
            (summed.at[2, pl.ds(64, 64)], arrived.at[1, pl.ds(64, 64)], left),
        )[number]
        return pltpu.make_async_remote_copy(
            here, there, sum_send.at[number], sum_recv.at[number],
            device_id=(s, target), device_id_type=MESH)

    def finish(step):
        if step == 3:
            stream[...] += 0.5 * chip_total(3)
        elif step == 0:
            summed[0] = chip_total(0).astype(jnp.bfloat16)
            sum_copy(0).start()
            sum_copy(1).start()
        else:
            total_rows = chip_total(step)
            sent, kept = (slice(64, 128), slice(0, 64)) if step == 1 else (slice(0, 64), slice(64, 128))
            summed[step, sent, :] = total_rows[sent].astype(jnp.bfloat16)
            sum_copy(step + 1).start()
            waiting[step - 1] = total_rows[kept]

    def mix(step, carry):
        @pl.when(step == 1)
        def _():
            row_wait(5)

        @pl.when(step == 2)
        def _():
            row_wait(6)

        chip = (x + pick(step, (2, 1, 3, 0))) % SIDE

        def columns(pair, first, count):
            return jnp.concatenate([weights_all[2 * pair + side, pl.ds(first, count), :] for side in range(2)], axis=1)

        def product(first, count):
            added = jnp.zeros((256, count), jnp.float32)
            for pair in range(8):
                rows = rows_all[pl.ds(2 * chip, 2), :, 256 * pair:256 * (pair + 1)].reshape(256, 256)
                added += lax.dot_general(
                    rows, columns(pair, first, count), (((1,), (1,)), ((), ())), preferred_element_type=jnp.float32)
            return added

        for first, count in ((0, 256), (256, 256), (512, 192)):
            gate_value, upward = product(first, count), product(UNITS + first, count)
            hidden[:, first:first + count] = (gate_value / (1.0 + jnp.exp(-gate_value)) * upward).astype(jnp.bfloat16)

        for one in range(3):
            @pl.when(step == one + 1)
            def _():
                finish(one)

        for pair in range(8):
            down = jnp.dot(hidden[...], columns(pair, 2 * UNITS, UNITS), preferred_element_type=jnp.float32)
            halves[step, :, :, 256 * pair:256 * (pair + 1)] = down.astype(jnp.bfloat16).reshape(2, 128, 256)
        part_copy(step).start()

        return carry

    lax.fori_loop(0, 4, mix, 0)
    for side in range(2):
        sum_copy(side).wait_recv()
        rows = pl.ds(64 * side, 64)
        summed[1 + side, rows, :] = (waiting[side] + relay[side].astype(jnp.float32)).astype(jnp.bfloat16)
        sum_copy(4 + side).start()
    finish(3)
    sum_copy(2).wait_recv()
    sum_copy(3).wait_recv()
    sum_copy(4).wait_recv()
    sum_copy(5).wait_recv()
    result[...] = (
        stream[...] + 0.5 * (arrived[0].astype(jnp.float32) + arrived[1].astype(jnp.float32))).astype(jnp.bfloat16)

    for number in range(6):
        sum_copy(number).wait_send()
    for step in range(4):
        part_copy(step).wait_send()
    for number in range(10):
        row_copy(number).wait_send()
    for number in range(14):
        out_copy(*out_sends[number]).wait_send()
    for copy in query_copies():
        copy.wait_send()
    for phase in range(len(SENDS)):
        for index in range(len(SENDS[phase])):
            shard_copy(0, phase, index).wait_send()
            shard_copy(1, phase, index).wait_send()
    for place in range(16):
        pair_copy(place).wait_send()
    for number in range(4):
        head_copy(1, number).wait_send()

        @pl.when(t != number)
        def _():
            head_copy(0, number).wait_send()


def layer_call(*operands):
    vmem = pl.BlockSpec(memory_space=pltpu.VMEM)
    anywhere = pl.BlockSpec(memory_space=pl.ANY)
    dma = pltpu.SemaphoreType.DMA
    bf16, f32 = jnp.bfloat16, jnp.float32
    return pl.pallas_call(
        layer_kernel,
        out_shape=jax.ShapeDtypeStruct((128, 2048), bf16),
        in_specs=[anywhere] * len(operands),
        out_specs=vmem,
        scratch_shapes=[
            pltpu.VMEM((ROWS, 256), bf16),
            pltpu.VMEM((ROWS, 128), bf16),
            pltpu.VMEM((HALF, 256), bf16),
            pltpu.VMEM((ROPE, HALF), bf16),
            pltpu.VMEM((1, 256), f32),
            pltpu.VMEM((256, 256), bf16),
            pltpu.VMEM((256, 256), bf16),
            pltpu.VMEM((128, 2048), bf16),
            pltpu.VMEM((1, 2048), f32),
            pltpu.VMEM((ROWS, 128), f32),
            pltpu.VMEM((ROWS, 128), f32),
            pltpu.VMEM((16, 128), f32),
            pltpu.VMEM((16, 128), f32),
            pltpu.VMEM((ROWS, 128), bf16),
            pltpu.VMEM((32, SHARD, 256), bf16),
            pltpu.VMEM((HALF, 256), bf16),
            pltpu.VMEM((HALF, 128), bf16),
            pltpu.VMEM((2, 2, 2, 256, HALF), bf16),
            pltpu.VMEM((2, ROWS, 256), bf16),
            pltpu.VMEM((256, ROWS), bf16),
            pltpu.VMEM((2, ROWS, 256), f32),
            pltpu.VMEM((256, 256), bf16),
            pltpu.VMEM((2, 2, 1, HALF), f32),
            pltpu.VMEM((2, 2, 1, HALF), f32),
            pltpu.VMEM((2, 2, VDIM, HALF), f32),
            pltpu.VMEM((2, HALF, 256), bf16),
            pltpu.VMEM((8, 128, 256), bf16),
            pltpu.VMEM((8, 256, 2048), bf16),
            pltpu.VMEM((16, 3 * UNITS, 128), bf16),
            pltpu.VMEM((256, UNITS), bf16),
            pltpu.VMEM((128, 2048), f32),
            pltpu.VMEM((8, 128, 2048), bf16),
            pltpu.VMEM((4, 2, 128, 2048), bf16),
            pltpu.VMEM((4, 128, 2048), bf16),
            pltpu.VMEM((3, 128, 2048), bf16),
            pltpu.VMEM((2, 64, 2048), bf16),
            pltpu.VMEM((2, 128, 2048), bf16),
            pltpu.VMEM((2, 64, 2048), f32),
            dma((32,)), dma((64,)), dma((16,)), dma((16,)), dma((2,)), dma((2,)),
            dma((8,)), dma((8,)), dma((14,)), dma((14,)), dma((4,)),
            dma((32,)), dma((64,)), dma((10,)), dma((10,)), dma((4,)), dma((4,)), dma((6,)), dma((6,)), dma((16,)),
        ],
        compiler_params=pltpu.CompilerParams(
            collective_id=0, has_side_effects=True, vmem_limit_bytes=67_000_000),
        cost_estimate=pl.CostEstimate(flops=60_000_000_000, bytes_accessed=30_000_000, transcendentals=18_000_000),
        name="layer",
    )(*operands)


def angle_tables(positions):
    frequency = theta_base ** (-2.0 * np.arange(ROPE // 2) / ROPE)
    angle = np.tile(np.asarray(positions, np.float64)[:, None] * frequency[None, :], (1, 4))
    return np.cos(angle).astype(np.float32), np.sin(angle).astype(np.float32)


def on_device(
    resid, query_nope, query_rope, latent, key_rope, latent_gain, w_key, w_value, w_out, mix_gain,
    w_gate, w_up, w_down,
):
    row_tables = angle_tables(np.arange(ROWS))
    block_tables = angle_tables(ROWS * np.arange(16))
    return layer_call(
        query_nope, query_rope, latent, key_rope.T, latent_gain.reshape(1, -1), w_key, w_value, w_out, resid,
        mix_gain.reshape(1, -1), w_gate.T, w_up.T, w_down.T,
        *(jnp.asarray(table) for table in row_tables + block_tables))


def solution(mesh):
    return jax.shard_map(
        on_device,
        mesh=mesh,
        in_specs=(
            P(("sp", "tp"), None),
            P("sp", "tp"),
            P("sp", "tp"),
            P("sp", None),
            P("sp", None),
            P(),
            P(None, "tp"),
            P(None, "tp"),
            P("tp", None),
            P(),
            P("sp", "tp"),
            P("sp", "tp"),
            P("sp", "tp"),
        ),
        out_specs=P(("sp", "tp"), None),
        check_vma=False,
    )
```

```python
import functools

import jax
import jax.numpy as jnp
import numpy as np
from jax import lax
from jax.experimental import pallas as pl
from jax.experimental.pallas import tpu as pltpu
from jax.sharding import PartitionSpec as P

NOPE = 128
ROPE = 64
VDIM = 128
ROWS = 1024
HALF = 512
SIDE = 4
UNITS = 704
SHARD = HALF + HALF // 4

norm_eps = 1e-06
masked_score = -1e30
theta_base = 10000.0
score_base2 = (NOPE + ROPE) ** (-0.5) * 1.4426950408889634
MESH = pl.DeviceIdType.MESH

ORDER = ((0, 0), (1, 0), (3, 0), (0, 1), (0, 3), (2, 0), (0, 2), (1, 1), (1, 3), (3, 1), (3, 3),
         (2, 1), (2, 3), (1, 2), (3, 2), (2, 2))
PLACE = {pair: p for p, pair in enumerate(ORDER)}
ALPHA, BETA, FULL = (0, 320), (320, 320), (0, 640)
ALPHA0, ALPHA1, BETA0, BETA1 = (0, 160), (160, 160), (320, 160), (480, 160)

SENDS = (
    (((0, 0), FULL, (1, 0), 0), ((0, 0), FULL, (-1, 0), 0), ((0, 0), FULL, (0, 1), 0), ((0, 0), FULL, (0, -1), 0)),
    (
        ((1, 0), ALPHA, (-1, 0), 0), ((3, 0), BETA, (1, 0), 1),
        ((0, 1), ALPHA, (0, -1), 0), ((0, 3), BETA, (0, 1), 1),
        ((1, 0), ALPHA, (0, 1), 0), ((1, 0), ALPHA, (0, -1), 0),
        ((3, 0), ALPHA, (0, 1), 0), ((3, 0), ALPHA, (0, -1), 0),
        ((0, 1), BETA, (1, 0), 1), ((0, 1), BETA, (-1, 0), 1),
        ((0, 3), BETA, (1, 0), 1), ((0, 3), BETA, (-1, 0), 1),
    ),
    (
        ((2, 0), ALPHA, (0, 1), 0), ((2, 0), ALPHA, (0, -1), 0),
        ((0, 2), BETA, (1, 0), 1), ((0, 2), BETA, (-1, 0), 1),
    ),
    (
        ((1, 1), ALPHA0, (0, -1), 0), ((1, 3), ALPHA1, (0, 1), 2),
        ((3, 1), ALPHA0, (0, -1), 0), ((3, 3), ALPHA1, (0, 1), 2),
        ((1, 1), BETA0, (-1, 0), 1), ((3, 1), BETA1, (1, 0), 2),
        ((1, 3), BETA0, (-1, 0), 1), ((3, 3), BETA1, (1, 0), 2),
    ),
    (
        ((2, 1), ALPHA0, (0, -1), 0), ((2, 3), ALPHA1, (0, 1), 1),
        ((1, 2), BETA0, (-1, 0), 2), ((3, 2), BETA1, (1, 0), 3),
    ),
)


def at_receiver(source, step):
    return PLACE[((source[0] - step[0]) % SIDE, (source[1] - step[1]) % SIDE)]


def pick(index, values):
    found = jnp.int32(values[0])
    for at in range(1, len(values)):
        found = jnp.where(index == at, jnp.int32(values[at]), found)
    return found


def layer_kernel(
    nope_in, rope_in, latent_in, key_in, gain_in, w_key_in, w_value_in, w_out, resid_in, mix_gain_in,
    gate_in, up_in, down_in, row_cos_in, row_sin_in, block_cos_in, block_sin_in, result,
    nope, rope, latent, key_rope, gain, w_key, w_value, resid, mix_gain,
    row_cos, row_sin, block_cos, block_sin, turned_queries,
    lat, far_nope, far_rope, queries, keys, values_t, held, w_value_t, top, total, acc, head_out,
    heads_all, w_out_all, weights_all, hidden, stream, rows_all, halves, got, summed, relay, arrived, waiting,
    send_sem, recv_sem, pair_send, pair_recv, query_send, query_recv, head_send, head_recv,
    out_send, out_recv, local_sem, mixer_send, mixer_recv, row_send, row_recv, part_send, part_recv,
    sum_send, sum_recv, load_sem,
):
    s = lax.axis_index("sp")
    t = lax.axis_index("tp")
    z, y = s // SIDE, s % SIDE
    x, core = t // 2, t % 2
    mirror = 15 - s

    def sp_at(dy, dz):
        return ((z + dz + SIDE) % SIDE) * SIDE + (y + dy + SIDE) % SIDE

    def tp_at(dx):
        return ((x + dx + SIDE) % SIDE) * 2 + core

    partner = x * 2 + 1 - core

    barrier = pltpu.get_barrier_semaphore()
    for step in (1, 2, 3):
        pl.semaphore_signal(barrier, inc=1, device_id=(sp_at(step, 0), t), device_id_type=MESH)
        pl.semaphore_signal(barrier, inc=1, device_id=(sp_at(0, step), t), device_id_type=MESH)
    for step in range(1, 8):
        pl.semaphore_signal(barrier, inc=1, device_id=(s, (t + step) % 8), device_id_type=MESH)
    for step in range(8):
        pl.semaphore_signal(barrier, inc=1, device_id=(mirror, (t + step) % 8), device_id_type=MESH)

    half_rows = pl.ds(pl.multiple_of(core * HALF, HALF), HALF)
    loads = [
        pltpu.make_async_copy(source, target, load_sem.at[number])
        for number, (source, target) in enumerate((
            (latent_in.at[half_rows], latent), (key_in.at[:, half_rows], key_rope), (gain_in, gain),
            (block_cos_in, block_cos), (block_sin_in, block_sin), (row_cos_in, row_cos), (row_sin_in, row_sin),
            *((rope_in.at[pl.ds(128 * one, 128)], rope.at[pl.ds(HALF * (one % 2) + 128 * (one // 2), 128)]) for one in range(8)),
            *((nope_in.at[pl.ds(128 * one, 128)], nope.at[pl.ds(HALF * (one % 2) + 128 * (one // 2), 128)]) for one in range(8)),
            (w_value_in, w_value), (w_key_in, w_key),
            (gate_in, weights_all.at[s, pl.ds(0, UNITS)]), (up_in, weights_all.at[s, pl.ds(UNITS, UNITS)]),
            (down_in, weights_all.at[s, pl.ds(2 * UNITS, UNITS)]), (resid_in, resid), (mix_gain_in, mix_gain),
        ))
    ]
    for load in loads:
        load.start()

    def rotated(rows_in, first):
        count = rows_in.shape[0]
        at = pl.ds(first, count)
        near_cos, near_sin = row_cos[at, :], row_sin[at, :]
        far_cos, far_sin = block_cos[pl.ds(s, 1), :], block_sin[pl.ds(s, 1), :]
        cosine = far_cos * near_cos - far_sin * near_sin
        sine = far_sin * near_cos + far_cos * near_sin
        lane = lax.broadcasted_iota(jnp.int32, rows_in.shape, 1) % ROPE
        swapped = jnp.where(lane < ROPE // 2, -pltpu.roll(rows_in, 96, 1), pltpu.roll(rows_in, 32, 1))
        return rows_in * cosine + swapped * sine

    own = 2 * s + core
    for load in loads[:7]:
        load.wait()
    wide = latent[...].astype(jnp.float32)
    scale = lax.rsqrt(jnp.mean(wide * wide, axis=-1, keepdims=True) + norm_eps)
    lat[own, pl.ds(0, HALF), :] = (wide * scale * gain[...]).astype(jnp.bfloat16)
    once = key_rope[...].astype(jnp.float32)
    twice = rotated(jnp.transpose(jnp.concatenate([once, once], axis=0)), core * HALF).astype(jnp.bfloat16)
    front_lanes = lax.broadcasted_iota(jnp.int32, (128, 128), 1) < ROPE
    for side in range(2):
        lat[own, pl.ds(HALF, 128), side * 128:(side + 1) * 128] = jnp.where(
            front_lanes, twice[128 * side:128 * side + 128], twice[256 + 128 * side:384 + 128 * side])
    for load in loads[7:23]:
        load.wait()
    for one in (1, 3, 5, 7, 0, 2, 4, 6):
        held_rows = pl.ds(HALF * (one % 2) + 128 * (one // 2), 128)
        turned_queries[held_rows, :] = rotated(
            rope[held_rows, :].astype(jnp.float32), 128 * one).astype(jnp.bfloat16)
    for load in loads[23:]:
        load.wait()
    pl.semaphore_wait(barrier, 21)

    def query_copies():
        return (
            pltpu.make_async_remote_copy(
                nope.at[pl.ds(HALF, HALF)], far_nope, query_send.at[0], query_recv.at[0],
                device_id=(mirror, t), device_id_type=MESH),
            pltpu.make_async_remote_copy(
                turned_queries.at[pl.ds(HALF, HALF)], far_rope, query_send.at[1], query_recv.at[1],
                device_id=(mirror, t), device_id_type=MESH),
        )

    def piece(kind, block, rows):
        first, count = rows
        if kind == 0:
            return lat.at[2 * block + core, pl.ds(first, count)]
        return weights_all.at[block, pl.ds(first * 33 // 10, count * 33 // 10)]

    def shard_copy(kind, phase, index):
        source, rows, step, slot = SENDS[phase][index]
        number = sum(len(one) for one in SENDS[:phase]) + index
        place = at_receiver(source, step)
        there = piece(kind, sp_at(*source), rows)
        return pltpu.make_async_remote_copy(
            there, there,
            (send_sem, mixer_send)[kind].at[number], (recv_sem, mixer_recv)[kind].at[4 * place + slot],
            device_id=(sp_at(*step), t), device_id_type=MESH)

    def start_phase(kind, phase, first_index=0, last_index=12):
        for index in range(len(SENDS[phase]))[first_index:last_index]:
            shard_copy(kind, phase, index).start()

    def wait_received(kind, phase, first_index=0, last_index=12):
        for source, rows, step, slot in SENDS[phase][first_index:last_index]:
            place = at_receiver(source, step)
            there = piece(kind, sp_at(*ORDER[place]), rows)
            pltpu.make_async_remote_copy(
                there, there,
                (send_sem, mixer_send)[kind].at[0], (recv_sem, mixer_recv)[kind].at[4 * place + slot],
                device_id=(sp_at(*step), t), device_id_type=MESH).wait_recv()

    def pair_copy(place):
        there = lat.at[2 * sp_at(*ORDER[place]) + core]
        return pltpu.make_async_remote_copy(
            there, there, pair_send.at[place], pair_recv.at[place],
            device_id=(s, partner), device_id_type=MESH)

    def hand_on(places):
        for place in places:
            pair_copy(place).start()

    def out_copy(number, slot, rows, target):
        first, count = rows
        source = w_out.at[pl.ds(first, count)] if number < 9 else w_out_all.at[slot, pl.ds(first, count)]
        return pltpu.make_async_remote_copy(
            source, w_out_all.at[slot, pl.ds(first, count)],
            out_send.at[number], out_recv.at[number],
            device_id=(s, target), device_id_type=MESH)

    whole, upper, lower = (0, 256), (0, 128), (128, 128)
    right, left, across = tp_at(1), tp_at(3), tp_at(2)
    chunks = tuple((64 * chunk, 64) for chunk in range(4))
    out_sends = (
        *((chunk, t, chunks[chunk], right) for chunk in range(4)),
        *((4 + chunk, t, chunks[chunk], left) for chunk in range(4)),
        (8, t, whole, partner),
        (9, right, upper, left), (10, left, lower, right),
        (11, right, whole, partner), (12, left, whole, partner), (13, across, whole, partner),
    )

    def other(slot):
        return (slot // 2) * 2 + 1 - slot % 2

    out_receives = (
        *((chunk, left, chunks[chunk]) for chunk in range(4)),
        *((4 + chunk, right, chunks[chunk]) for chunk in range(4)),
        (8, partner, whole),
        (9, across, upper), (10, across, lower),
        (11, other(right), whole), (12, other(left), whole), (13, other(across), whole),
    )

    def out_chunk(chunk):
        out_copy(*out_sends[3 - chunk]).start()
        out_copy(*out_sends[4 + chunk]).start()

    def out_wait(number):
        _, slot, (first, count) = out_receives[number]
        pltpu.make_async_remote_copy(
            w_out_all.at[slot, pl.ds(first, count)], w_out_all.at[slot, pl.ds(first, count)],
            out_send.at[number], out_recv.at[number],
            device_id=(s, partner), device_id_type=MESH).wait_recv()

    start_phase(0, 0)
    for copy in query_copies():
        copy.start()
    out_copy(*out_sends[8]).start()
    own_out = pltpu.make_async_copy(w_out, w_out_all.at[t], local_sem.at[1])
    own_out.start()

    w_value_t[...] = jnp.transpose(w_value[...].astype(jnp.float32)).astype(jnp.bfloat16)
    top[...] = jnp.full_like(top, masked_score)
    total[...] = jnp.zeros_like(total)
    acc[...] = jnp.zeros_like(acc)

    lanes = lax.broadcasted_iota(jnp.int32, (HALF, 128), 1)

    def set_queries(group, nope_rows, rope_rows):
        wide = rope_rows.astype(jnp.float32)
        turned = pltpu.roll(wide, 64, 1)
        front = lanes < 64
        for head in range(2):
            one = jnp.transpose(nope_rows[:, head * NOPE:(head + 1) * NOPE].astype(jnp.float32))
            low, high = (wide, turned) if head == 0 else (turned, wide)
            for version, tail in enumerate((jnp.where(front, low, 0.0), jnp.where(front, 0.0, high))):
                queries[group, head, version, 0:NOPE, :] = one.astype(jnp.bfloat16)
                queries[group, head, version, NOPE:2 * NOPE, :] = jnp.transpose(tail).astype(jnp.bfloat16)

    hand_on((0,))
    for chunk in range(4):
        out_chunk(chunk)
    set_queries(0, nope[pl.ds(0, HALF), :], turned_queries[pl.ds(0, HALF), :])

    def expand(block):
        for plane in range(2):
            rows = lat[2 * block + plane, pl.ds(0, HALF), :]
            expanded = jnp.dot(rows, w_key[...], preferred_element_type=jnp.float32).astype(jnp.bfloat16)
            tails = tuple(lat[2 * block + plane, pl.ds(HALF, 128), side * 128:(side + 1) * 128] for side in range(2))
            for head in range(2):
                keys[head, pl.ds(plane * HALF, HALF), 0:NOPE] = expanded[:, head * NOPE:(head + 1) * NOPE]
                for quarter in range(4):
                    keys[head, pl.ds(plane * HALF + quarter * 128, 128), NOPE:2 * NOPE] = tails[quarter % 2]
            values_t[:, plane * HALF:(plane + 1) * HALF] = lax.dot_general(
                w_value_t[...], rows, (((1,), (1,)), ((), ())), preferred_element_type=jnp.float32
            ).astype(jnp.bfloat16)

    def fold(group, masked):
        def make(piece_at):
            head, first = piece_at // 2, (piece_at % 2) * 256
            largest = top[group, head, :, first:first + 256]
            for chunk in range(4):
                scores = jnp.dot(
                    keys[head, pl.ds(256 * chunk, 256), :],
                    queries[group, head, chunk % 2, :, first:first + 256],
                    preferred_element_type=jnp.float32)
                if masked:
                    key_at = lax.broadcasted_iota(jnp.int32, scores.shape, 0) + 256 * chunk
                    column = lax.broadcasted_iota(jnp.int32, scores.shape, 1)
                    query_at = column + jnp.where(column >= 128, 128, 0) + (2 * first + 128 * group)
                    scores = jnp.where(key_at <= query_at, scores, masked_score)
                held[piece_at % 2, pl.ds(256 * chunk, 256), :] = scores
                largest = jnp.maximum(largest, jnp.max(scores, axis=0, keepdims=True))
            return largest

        after = make(0)
        for piece_at in range(4):
            following = make(piece_at + 1) if piece_at < 3 else None
            head, first = piece_at // 2, (piece_at % 2) * 256
            columns = slice(first, first + 256)
            before = top[group, head, :, columns]
            offset = after * score_base2
            added = jnp.zeros((1, 256), jnp.float32)
            mixed = jnp.zeros((VDIM, 256), jnp.float32)
            for chunk in range(4):
                weights = jnp.exp2(held[piece_at % 2, pl.ds(256 * chunk, 256), :] * score_base2 - offset)
                added += jnp.sum(weights, axis=0, keepdims=True)
                mixed += jnp.dot(
                    values_t[head * VDIM:(head + 1) * VDIM, 256 * chunk:256 * (chunk + 1)],
                    weights.astype(jnp.bfloat16), preferred_element_type=jnp.float32)
            factor = jnp.exp2((before - after) * score_base2)
            total[group, head, :, columns] = total[group, head, :, columns] * factor + added
            acc[group, head, :, columns] = acc[group, head, :, columns] * factor + mixed
            top[group, head, :, columns] = after
            after = following

    def process(block, place):
        @pl.when(block <= jnp.maximum(s, mirror))
        def _():
            expand(block)

        def one(group, carry):
            last = jnp.where(group == 0, s, mirror)

            @pl.when((place == 0) & (group == 1))
            def _():
                wait_received(0, 0)
                start_phase(0, 1)
                hand_on((1, 2, 3, 4))
                for copy in query_copies():
                    copy.wait_recv()
                set_queries(1, far_nope[...], far_rope[...])

            @pl.when(block < last)
            def _():
                fold(group, False)

            @pl.when(block == last)
            def _():
                fold(group, True)

            return carry

        lax.fori_loop(0, 2, one, 0)

    def advance(place, carry):
        @pl.when(place == 1)
        def _():
            wait_received(0, 1, 0, 4)
            start_phase(0, 2)
            hand_on((5, 6))

        @pl.when(place == 3)
        def _():
            wait_received(0, 1, 4, 12)
            start_phase(0, 3)
            hand_on((7, 8, 9, 10))
            start_phase(1, 0)

        @pl.when(place == 6)
        def _():
            wait_received(0, 2)
            wait_received(0, 3)
            start_phase(0, 4)
            hand_on((11, 12, 13, 14))
            for number in (2, 3, 4, 5):
                out_wait(number)
            for number in (9, 10):
                out_copy(*out_sends[number]).start()

        @pl.when(place == 10)
        def _():
            for number in (0, 1, 6, 7):
                out_wait(number)
            for number in (11, 12):
                out_copy(*out_sends[number]).start()

        @pl.when(place == 12)
        def _():
            wait_received(1, 0)
            start_phase(1, 1, 0, 4)
            start_phase(1, 1, 4, 6)
            start_phase(1, 1, 8, 10)

        @pl.when(place == 13)
        def _():
            wait_received(0, 4)
            hand_on((15,))
            for number in (9, 10):
                out_wait(number)
            out_copy(*out_sends[13]).start()

        dy = pick(place, [pair[0] for pair in ORDER])
        dz = pick(place, [pair[1] for pair in ORDER])
        block = sp_at(dy, dz)
        theirs = lat.at[2 * block + 1 - core]
        pltpu.make_async_remote_copy(
            theirs, theirs, pair_send.at[place], pair_recv.at[place],
            device_id=(s, partner), device_id_type=MESH).wait_recv()
        process(block, place)
        return carry

    lax.fori_loop(0, 16, advance, 0)

    def head_copy(group, part):
        target = 2 * part + group
        return pltpu.make_async_remote_copy(
            head_out.at[group, pl.ds(128 * part, 128)], heads_all.at[t],
            head_send.at[4 * group + part], head_recv.at[t],
            device_id=(s if group == 0 else mirror, target), device_id_type=MESH)

    def close(group):
        for head in range(2):
            mixed = acc[group, head] / total[group, head]
            head_out[group, :, head * VDIM:(head + 1) * VDIM] = jnp.transpose(mixed).astype(jnp.bfloat16)

    close(1)
    for number in range(4):
        head_copy(1, number).start()
    close(0)
    for number in range(4):
        @pl.when(t != 2 * number)
        def _():
            head_copy(0, number).start()

    @pl.when(core == 0)
    def _():
        mine = pltpu.make_async_copy(
            head_out.at[0, pl.ds(128 * x, 128)], heads_all.at[t], local_sem.at[2])
        mine.start()
        mine.wait()

    def head_wait(slot):
        @pl.when((core == 1) | (slot != t))
        def _():
            pltpu.make_async_remote_copy(
                head_out.at[0, pl.ds(0, 128)], heads_all.at[slot], head_send.at[0], head_recv.at[slot],
                device_id=(mirror, t), device_id_type=MESH).wait_recv()

    start_phase(1, 1, 6, 8)
    start_phase(1, 1, 10, 12)
    wait_received(1, 1, 0, 4)
    start_phase(1, 2)
    for number in (8, 11, 12, 13):
        out_wait(number)
    own_out.wait()

    stream[...] = resid[...].astype(jnp.float32)

    def project(turn, carry):
        slot = pick(turn, (0, 1, 2, 3, 6, 7, 4, 5))
        slot = (2 * x + core + slot - 2 * ((core + slot % 2) // 2)) % 8
        head_wait(slot)
        stream[...] += jnp.dot(heads_all[slot], w_out_all[slot], preferred_element_type=jnp.float32)
        return carry

    lax.fori_loop(0, 8, project, 0)
    rows_f32 = stream[...]
    scale = lax.rsqrt(jnp.mean(rows_f32 * rows_f32, axis=-1, keepdims=True) + norm_eps)
    rows_all[t] = (rows_f32 * scale * mix_gain[...]).astype(jnp.bfloat16)

    high, low = (0, 64), (64, 64)
    all_rows = (0, 128)
    row_sends = (
        (0, t, low, right), (1, t, high, left), (2, t, all_rows, partner),
        (3, right, high, left), (4, left, low, right),
        (5, right, all_rows, partner), (6, left, all_rows, partner), (7, across, all_rows, partner),
        (8, t, high, right), (9, t, low, left),
    )
    row_receives = (
        (0, left, low), (1, right, high), (2, partner, all_rows),
        (3, across, high), (4, across, low),
        (5, other(right), all_rows), (6, other(left), all_rows), (7, other(across), all_rows),
        (8, left, high), (9, right, low),
    )

    def row_copy(number):
        _, slot, (first, count), target = row_sends[number]
        here = rows_all.at[slot, pl.ds(first, count)]
        return pltpu.make_async_remote_copy(
            here, here, row_send.at[number], row_recv.at[number],
            device_id=(s, target), device_id_type=MESH)

    def row_wait(number):
        _, slot, (first, count) = row_receives[number]
        here = rows_all.at[slot, pl.ds(first, count)]
        pltpu.make_async_remote_copy(
            here, here, row_send.at[number], row_recv.at[number],
            device_id=(s, partner), device_id_type=MESH).wait_recv()

    for number in range(3):
        row_copy(number).start()
    wait_received(1, 1, 4, 12)
    start_phase(1, 3)
    row_wait(0)
    row_wait(1)
    for number in (3, 4, 8, 9):
        row_copy(number).start()
    wait_received(1, 2)
    wait_received(1, 3)
    start_phase(1, 4)
    row_wait(2)
    row_wait(3)
    row_wait(4)
    row_copy(7).start()
    wait_received(1, 4)
    row_wait(7)

    def part_copy(step):
        return pltpu.make_async_remote_copy(
            halves.at[step, 1 - core], got.at[step], part_send.at[step], part_recv.at[step],
            device_id=(s, partner), device_id_type=MESH)

    def chip_total(step):
        part_copy(step).wait_recv()
        return halves[step, core].astype(jnp.float32) + got[step].astype(jnp.float32)

    def sum_copy(number):
        here, there, target = (
            (summed.at[0, pl.ds(0, 64)], relay.at[0], right),
            (summed.at[0, pl.ds(64, 64)], relay.at[1], left),
            (summed.at[1, pl.ds(64, 64)], arrived.at[0, pl.ds(64, 64)], right),
            (summed.at[2, pl.ds(0, 64)], arrived.at[1, pl.ds(0, 64)], left),
            (summed.at[1, pl.ds(0, 64)], arrived.at[0, pl.ds(0, 64)], right),
            (summed.at[2, pl.ds(64, 64)], arrived.at[1, pl.ds(64, 64)], left),
        )[number]
        return pltpu.make_async_remote_copy(
            here, there, sum_send.at[number], sum_recv.at[number],
            device_id=(s, target), device_id_type=MESH)

    def finish(step):
        if step == 3:
            stream[...] += 0.5 * chip_total(3)
        elif step == 0:
            summed[0] = chip_total(0).astype(jnp.bfloat16)
            sum_copy(0).start()
            sum_copy(1).start()
        else:
            total_rows = chip_total(step)
            sent, kept = (slice(64, 128), slice(0, 64)) if step == 1 else (slice(0, 64), slice(64, 128))
            summed[step, sent, :] = total_rows[sent].astype(jnp.bfloat16)
            sum_copy(step + 1).start()
            waiting[step - 1] = total_rows[kept]

    def mix(step, carry):
        @pl.when(step == 1)
        def _():
            row_wait(8)
            row_wait(9)
            row_copy(5).start()
            row_copy(6).start()
            row_wait(5)

        @pl.when(step == 2)
        def _():
            row_wait(6)

        chip = (x + pick(step, (2, 1, 3, 0))) % SIDE

        def columns(pair, first, count):
            return jnp.concatenate([weights_all[2 * pair + side, pl.ds(first, count), :] for side in range(2)], axis=1)

        def product(first, count):
            added = jnp.zeros((256, count), jnp.float32)
            for pair in range(8):
                rows = rows_all[pl.ds(2 * chip, 2), :, 256 * pair:256 * (pair + 1)].reshape(256, 256)
                added += lax.dot_general(
                    rows, columns(pair, first, count), (((1,), (1,)), ((), ())), preferred_element_type=jnp.float32)
            return added

        for first, count in ((0, 256), (256, 256), (512, 192)):
            gate_value, upward = product(first, count), product(UNITS + first, count)
            hidden[:, first:first + count] = (gate_value / (1.0 + jnp.exp(-gate_value)) * upward).astype(jnp.bfloat16)

        for one in range(3):
            @pl.when(step == one + 1)
            def _():
                finish(one)

        for pair in range(8):
            down = jnp.dot(hidden[...], columns(pair, 2 * UNITS, UNITS), preferred_element_type=jnp.float32)
            halves[step, :, :, 256 * pair:256 * (pair + 1)] = down.astype(jnp.bfloat16).reshape(2, 128, 256)
        part_copy(step).start()

        return carry

    lax.fori_loop(0, 4, mix, 0)
    for side in range(2):
        sum_copy(side).wait_recv()
        rows = pl.ds(64 * side, 64)
        summed[1 + side, rows, :] = (waiting[side] + relay[side].astype(jnp.float32)).astype(jnp.bfloat16)
        sum_copy(4 + side).start()
    finish(3)
    sum_copy(2).wait_recv()
    sum_copy(3).wait_recv()
    sum_copy(4).wait_recv()
    sum_copy(5).wait_recv()
    result[...] = (
        stream[...] + 0.5 * (arrived[0].astype(jnp.float32) + arrived[1].astype(jnp.float32))).astype(jnp.bfloat16)

    for number in range(6):
        sum_copy(number).wait_send()
    for step in range(4):
        part_copy(step).wait_send()
    for number in range(10):
        row_copy(number).wait_send()
    for number in range(14):
        out_copy(*out_sends[number]).wait_send()
    for copy in query_copies():
        copy.wait_send()
    for phase in range(len(SENDS)):
        for index in range(len(SENDS[phase])):
            shard_copy(0, phase, index).wait_send()
            shard_copy(1, phase, index).wait_send()
    for place in range(16):
        pair_copy(place).wait_send()
    for number in range(4):
        head_copy(1, number).wait_send()

        @pl.when(t != 2 * number)
        def _():
            head_copy(0, number).wait_send()


def layer_call(*operands):
    vmem = pl.BlockSpec(memory_space=pltpu.VMEM)
    anywhere = pl.BlockSpec(memory_space=pl.ANY)
    dma = pltpu.SemaphoreType.DMA
    bf16, f32 = jnp.bfloat16, jnp.float32
    return pl.pallas_call(
        layer_kernel,
        out_shape=jax.ShapeDtypeStruct((128, 2048), bf16),
        in_specs=[anywhere] * len(operands),
        out_specs=vmem,
        scratch_shapes=[
            pltpu.VMEM((ROWS, 256), bf16),
            pltpu.VMEM((ROWS, 128), bf16),
            pltpu.VMEM((HALF, 256), bf16),
            pltpu.VMEM((ROPE, HALF), bf16),
            pltpu.VMEM((1, 256), f32),
            pltpu.VMEM((256, 256), bf16),
            pltpu.VMEM((256, 256), bf16),
            pltpu.VMEM((128, 2048), bf16),
            pltpu.VMEM((1, 2048), f32),
            pltpu.VMEM((ROWS, 128), f32),
            pltpu.VMEM((ROWS, 128), f32),
            pltpu.VMEM((16, 128), f32),
            pltpu.VMEM((16, 128), f32),
            pltpu.VMEM((ROWS, 128), bf16),
            pltpu.VMEM((32, SHARD, 256), bf16),
            pltpu.VMEM((HALF, 256), bf16),
            pltpu.VMEM((HALF, 128), bf16),
            pltpu.VMEM((2, 2, 2, 256, HALF), bf16),
            pltpu.VMEM((2, ROWS, 256), bf16),
            pltpu.VMEM((256, ROWS), bf16),
            pltpu.VMEM((2, ROWS, 256), f32),
            pltpu.VMEM((256, 256), bf16),
            pltpu.VMEM((2, 2, 1, HALF), f32),
            pltpu.VMEM((2, 2, 1, HALF), f32),
            pltpu.VMEM((2, 2, VDIM, HALF), f32),
            pltpu.VMEM((2, HALF, 256), bf16),
            pltpu.VMEM((8, 128, 256), bf16),
            pltpu.VMEM((8, 256, 2048), bf16),
            pltpu.VMEM((16, 3 * UNITS, 128), bf16),
            pltpu.VMEM((256, UNITS), bf16),
            pltpu.VMEM((128, 2048), f32),
            pltpu.VMEM((8, 128, 2048), bf16),
            pltpu.VMEM((4, 2, 128, 2048), bf16),
            pltpu.VMEM((4, 128, 2048), bf16),
            pltpu.VMEM((3, 128, 2048), bf16),
            pltpu.VMEM((2, 64, 2048), bf16),
            pltpu.VMEM((2, 128, 2048), bf16),
            pltpu.VMEM((2, 64, 2048), f32),
            dma((32,)), dma((64,)), dma((16,)), dma((16,)), dma((2,)), dma((2,)),
            dma((8,)), dma((8,)), dma((14,)), dma((14,)), dma((4,)),
            dma((32,)), dma((64,)), dma((10,)), dma((10,)), dma((4,)), dma((4,)), dma((6,)), dma((6,)), dma((30,)),
        ],
        compiler_params=pltpu.CompilerParams(
            collective_id=0, has_side_effects=True, vmem_limit_bytes=67_000_000),
        cost_estimate=pl.CostEstimate(flops=60_000_000_000, bytes_accessed=30_000_000, transcendentals=18_000_000),
        name="layer",
    )(*operands)


def angle_tables(positions):
    frequency = theta_base ** (-2.0 * np.arange(ROPE // 2) / ROPE)
    angle = np.tile(np.asarray(positions, np.float64)[:, None] * frequency[None, :], (1, 4))
    return np.cos(angle).astype(np.float32), np.sin(angle).astype(np.float32)


def on_device(
    resid, query_nope, query_rope, latent, key_rope, latent_gain, w_key, w_value, w_out, mix_gain,
    w_gate, w_up, w_down,
):
    row_tables = angle_tables(np.arange(ROWS))
    block_tables = angle_tables(ROWS * np.arange(16))
    return layer_call(
        query_nope, query_rope, latent, key_rope.T, latent_gain.reshape(1, -1), w_key, w_value, w_out, resid,
        mix_gain.reshape(1, -1), w_gate.T, w_up.T, w_down.T,
        *(jnp.asarray(table) for table in row_tables + block_tables))


def solution(mesh):
    return jax.shard_map(
        on_device,
        mesh=mesh,
        in_specs=(
            P(("sp", "tp"), None),
            P("sp", "tp"),
            P("sp", "tp"),
            P("sp", None),
            P("sp", None),
            P(),
            P(None, "tp"),
            P(None, "tp"),
            P("tp", None),
            P(),
            P("sp", "tp"),
            P("sp", "tp"),
            P("sp", "tp"),
        ),
        out_specs=P(("sp", "tp"), None),
        check_vma=False,
    )
```

```python
import functools

import jax
import jax.numpy as jnp
import numpy as np
from jax import lax
from jax.experimental import pallas as pl
from jax.experimental.pallas import tpu as pltpu
from jax.sharding import PartitionSpec as P

NOPE = 128
ROPE = 64
VDIM = 128
ROWS = 1024
HALF = 512
SIDE = 4
UNITS = 704
SHARD = HALF + HALF // 4

norm_eps = 1e-06
masked_score = -1e30
theta_base = 10000.0
score_base2 = (NOPE + ROPE) ** (-0.5) * 1.4426950408889634
MESH = pl.DeviceIdType.MESH

ORDER = ((0, 0), (1, 0), (3, 0), (0, 1), (0, 3), (2, 0), (0, 2), (1, 1), (1, 3), (3, 1), (3, 3),
         (2, 1), (2, 3), (1, 2), (3, 2), (2, 2))
PLACE = {pair: p for p, pair in enumerate(ORDER)}
ALPHA, BETA, FULL = (0, 320), (320, 320), (0, 640)
ALPHA0, ALPHA1, BETA0, BETA1 = (0, 160), (160, 160), (320, 160), (480, 160)

SENDS = (
    (((0, 0), FULL, (1, 0), 0), ((0, 0), FULL, (-1, 0), 0), ((0, 0), FULL, (0, 1), 0), ((0, 0), FULL, (0, -1), 0)),
    (
        ((1, 0), ALPHA, (-1, 0), 0), ((3, 0), BETA, (1, 0), 1),
        ((0, 1), ALPHA, (0, -1), 0), ((0, 3), BETA, (0, 1), 1),
        ((1, 0), ALPHA, (0, 1), 0), ((1, 0), ALPHA, (0, -1), 0),
        ((3, 0), ALPHA, (0, 1), 0), ((3, 0), ALPHA, (0, -1), 0),
        ((0, 1), BETA, (1, 0), 1), ((0, 1), BETA, (-1, 0), 1),
        ((0, 3), BETA, (1, 0), 1), ((0, 3), BETA, (-1, 0), 1),
    ),
    (
        ((2, 0), ALPHA, (0, 1), 0), ((2, 0), ALPHA, (0, -1), 0),
        ((0, 2), BETA, (1, 0), 1), ((0, 2), BETA, (-1, 0), 1),
    ),
    (
        ((1, 1), ALPHA0, (0, -1), 0), ((1, 3), ALPHA1, (0, 1), 2),
        ((3, 1), ALPHA0, (0, -1), 0), ((3, 3), ALPHA1, (0, 1), 2),
        ((1, 1), BETA0, (-1, 0), 1), ((3, 1), BETA1, (1, 0), 2),
        ((1, 3), BETA0, (-1, 0), 1), ((3, 3), BETA1, (1, 0), 2),
    ),
    (
        ((2, 1), ALPHA0, (0, -1), 0), ((2, 3), ALPHA1, (0, 1), 1),
        ((1, 2), BETA0, (-1, 0), 2), ((3, 2), BETA1, (1, 0), 3),
    ),
)


def at_receiver(source, step):
    return PLACE[((source[0] - step[0]) % SIDE, (source[1] - step[1]) % SIDE)]


def pick(index, values):
    found = jnp.int32(values[0])
    for at in range(1, len(values)):
        found = jnp.where(index == at, jnp.int32(values[at]), found)
    return found


def layer_kernel(
    nope_in, rope_in, latent_in, key_in, gain_in, w_key_in, w_value_in, w_out, resid_in, mix_gain_in,
    gate_in, up_in, down_in, row_cos_in, row_sin_in, block_cos_in, block_sin_in, result,
    nope, rope, latent, key_rope, gain, w_key, w_value, resid, mix_gain,
    row_cos, row_sin, block_cos, block_sin, turned_queries,
    lat, far_nope, far_rope, queries, keys, values_t, held, w_value_t, top, total, acc, head_out,
    heads_all, w_out_all, weights_all, hidden, stream, rows_all, halves, got, summed, relay, arrived, waiting,
    send_sem, recv_sem, side_send, side_recv, pair_send, pair_recv, query_send, query_recv, head_send, head_recv,
    out_send, out_recv, local_sem, mixer_send, mixer_recv, row_send, row_recv, part_send, part_recv,
    sum_send, sum_recv, load_sem,
):
    s = lax.axis_index("sp")
    t = lax.axis_index("tp")
    z, y = s // SIDE, s % SIDE
    x, core = t // 2, t % 2
    mirror = 15 - s

    def sp_at(dy, dz):
        return ((z + dz + SIDE) % SIDE) * SIDE + (y + dy + SIDE) % SIDE

    def tp_at(dx):
        return ((x + dx + SIDE) % SIDE) * 2 + core

    partner = x * 2 + 1 - core

    barrier = pltpu.get_barrier_semaphore()
    for step in (1, 2, 3):
        pl.semaphore_signal(barrier, inc=1, device_id=(sp_at(step, 0), t), device_id_type=MESH)
        pl.semaphore_signal(barrier, inc=1, device_id=(sp_at(0, step), t), device_id_type=MESH)
    for step in range(1, 8):
        pl.semaphore_signal(barrier, inc=1, device_id=(s, (t + step) % 8), device_id_type=MESH)
    for step in range(8):
        pl.semaphore_signal(barrier, inc=1, device_id=(mirror, (t + step) % 8), device_id_type=MESH)

    half_rows = pl.ds(pl.multiple_of(core * HALF, HALF), HALF)
    loads = [
        pltpu.make_async_copy(source, target, load_sem.at[number])
        for number, (source, target) in enumerate((
            (latent_in.at[half_rows], latent), (key_in.at[:, half_rows], key_rope), (gain_in, gain),
            (block_cos_in, block_cos), (block_sin_in, block_sin), (row_cos_in, row_cos), (row_sin_in, row_sin),
            *((rope_in.at[pl.ds(128 * one, 128)], rope.at[pl.ds(HALF * (one % 2) + 128 * (one // 2), 128)]) for one in range(8)),
            *((nope_in.at[pl.ds(128 * one, 128)], nope.at[pl.ds(HALF * (one % 2) + 128 * (one // 2), 128)]) for one in range(8)),
            (w_value_in, w_value), (w_key_in, w_key),
            (gate_in, weights_all.at[s, pl.ds(0, UNITS)]), (up_in, weights_all.at[s, pl.ds(UNITS, UNITS)]),
            (down_in, weights_all.at[s, pl.ds(2 * UNITS, UNITS)]), (resid_in, resid), (mix_gain_in, mix_gain),
        ))
    ]
    for load in loads:
        load.start()

    def rotated(rows_in, first):
        count = rows_in.shape[0]
        at = pl.ds(first, count)
        near_cos, near_sin = row_cos[at, :], row_sin[at, :]
        far_cos, far_sin = block_cos[pl.ds(s, 1), :], block_sin[pl.ds(s, 1), :]
        cosine = far_cos * near_cos - far_sin * near_sin
        sine = far_sin * near_cos + far_cos * near_sin
        lane = lax.broadcasted_iota(jnp.int32, rows_in.shape, 1) % ROPE
        swapped = jnp.where(lane < ROPE // 2, -pltpu.roll(rows_in, 96, 1), pltpu.roll(rows_in, 32, 1))
        return rows_in * cosine + swapped * sine

    own = 2 * s + core
    for load in loads[:7]:
        load.wait()
    wide = latent[...].astype(jnp.float32)
    scale = lax.rsqrt(jnp.mean(wide * wide, axis=-1, keepdims=True) + norm_eps)
    lat[own, pl.ds(0, HALF), :] = (wide * scale * gain[...]).astype(jnp.bfloat16)
    once = key_rope[...].astype(jnp.float32)
    twice = rotated(jnp.transpose(jnp.concatenate([once, once], axis=0)), core * HALF).astype(jnp.bfloat16)
    front_lanes = lax.broadcasted_iota(jnp.int32, (128, 128), 1) < ROPE
    for side in range(2):
        lat[own, pl.ds(HALF, 128), side * 128:(side + 1) * 128] = jnp.where(
            front_lanes, twice[128 * side:128 * side + 128], twice[256 + 128 * side:384 + 128 * side])
    for load in loads[7:23]:
        load.wait()
    for one in (1, 3, 5, 7, 0, 2, 4, 6):
        held_rows = pl.ds(HALF * (one % 2) + 128 * (one // 2), 128)
        turned_queries[held_rows, :] = rotated(
            rope[held_rows, :].astype(jnp.float32), 128 * one).astype(jnp.bfloat16)
    for load in loads[23:]:
        load.wait()
    pl.semaphore_wait(barrier, 21)

    def query_copies():
        return (
            pltpu.make_async_remote_copy(
                nope.at[pl.ds(HALF, HALF)], far_nope, query_send.at[0], query_recv.at[0],
                device_id=(mirror, t), device_id_type=MESH),
            pltpu.make_async_remote_copy(
                turned_queries.at[pl.ds(HALF, HALF)], far_rope, query_send.at[1], query_recv.at[1],
                device_id=(mirror, t), device_id_type=MESH),
        )

    even_odd = x % 2

    def piece(kind, block, rows, split=False):
        first, count = rows
        if kind == 0:
            if split:
                first = first // 320 * 320 + 160 * even_odd + (first % 320) // 2
                return lat.at[2 * block + core, pl.ds(pl.multiple_of(first, 16), count // 2)]
            return lat.at[2 * block + core, pl.ds(first, count)]
        return weights_all.at[block, pl.ds(first * 33 // 10, count * 33 // 10)]

    def shard_copy(kind, phase, index):
        source, rows, step, slot = SENDS[phase][index]
        number = sum(len(one) for one in SENDS[:phase]) + index
        place = at_receiver(source, step)
        there = piece(kind, sp_at(*source), rows, phase > 1 or phase == 1 and index > 3)
        return pltpu.make_async_remote_copy(
            there, there,
            (send_sem, mixer_send)[kind].at[number], (recv_sem, mixer_recv)[kind].at[4 * place + slot],
            device_id=(sp_at(*step), t), device_id_type=MESH)

    def start_phase(kind, phase, first_index=0, last_index=12):
        for index in range(len(SENDS[phase]))[first_index:last_index]:
            shard_copy(kind, phase, index).start()

    def wait_received(kind, phase, first_index=0, last_index=12):
        for index, (source, rows, step, slot) in list(enumerate(SENDS[phase]))[first_index:last_index]:
            place = at_receiver(source, step)
            there = piece(kind, sp_at(*ORDER[place]), rows, phase > 1 or phase == 1 and index > 3)
            pltpu.make_async_remote_copy(
                there, there,
                (send_sem, mixer_send)[kind].at[0], (recv_sem, mixer_recv)[kind].at[4 * place + slot],
                device_id=(sp_at(*step), t), device_id_type=MESH).wait_recv()

    def pair_copy(place):
        there = lat.at[2 * sp_at(*ORDER[place]) + core]
        return pltpu.make_async_remote_copy(
            there, there, pair_send.at[place], pair_recv.at[place],
            device_id=(s, partner), device_id_type=MESH)

    def hand_on(places):
        for place in places:
            if place < 7:
                pair_copy(place).start()
            else:
                side_copy(place, 0).start()
                side_copy(place, 1).start()

    def side_copy(place, part):
        there = piece(0, sp_at(*ORDER[place]), (ALPHA, BETA)[part], True)
        number = 2 * (place - 7) + part
        return pltpu.make_async_remote_copy(
            there, there, side_send.at[number], side_recv.at[number],
            device_id=(s, tp_at(1 - 2 * core)), device_id_type=MESH)

    def side_arrived(place):
        block = 2 * sp_at(pick(place, [pair[0] for pair in ORDER]), pick(place, [pair[1] for pair in ORDER])) + core
        for part in range(2):
            first = pl.multiple_of(320 * part + 160 * (1 - even_odd), 16)
            there = lat.at[block, pl.ds(first, 160)]
            number = 2 * (place - 7) + part
            pltpu.make_async_remote_copy(
                there, there, side_send.at[number], side_recv.at[number],
                device_id=(s, partner), device_id_type=MESH).wait_recv()
        pltpu.make_async_remote_copy(
            lat.at[block], lat.at[block], pair_send.at[place], pair_recv.at[place],
            device_id=(s, partner), device_id_type=MESH).start()

    def out_copy(number, slot, rows, target):
        first, count = rows
        source = w_out.at[pl.ds(first, count)] if number < 9 else w_out_all.at[slot, pl.ds(first, count)]
        return pltpu.make_async_remote_copy(
            source, w_out_all.at[slot, pl.ds(first, count)],
            out_send.at[number], out_recv.at[number],
            device_id=(s, target), device_id_type=MESH)

    whole, upper, lower = (0, 256), (0, 128), (128, 128)
    right, left, across = tp_at(1), tp_at(3), tp_at(2)
    chunks = tuple((64 * chunk, 64) for chunk in range(4))
    out_sends = (
        *((chunk, t, chunks[chunk], right) for chunk in range(4)),
        *((4 + chunk, t, chunks[chunk], left) for chunk in range(4)),
        (8, t, whole, partner),
        (9, right, upper, left), (10, left, lower, right),
        (11, right, whole, partner), (12, left, whole, partner), (13, across, whole, partner),
    )

    def other(slot):
        return (slot // 2) * 2 + 1 - slot % 2

    out_receives = (
        *((chunk, left, chunks[chunk]) for chunk in range(4)),
        *((4 + chunk, right, chunks[chunk]) for chunk in range(4)),
        (8, partner, whole),
        (9, across, upper), (10, across, lower),
        (11, other(right), whole), (12, other(left), whole), (13, other(across), whole),
    )

    def out_chunk(chunk):
        out_copy(*out_sends[3 - chunk]).start()
        out_copy(*out_sends[4 + chunk]).start()

    def out_wait(number):
        _, slot, (first, count) = out_receives[number]
        pltpu.make_async_remote_copy(
            w_out_all.at[slot, pl.ds(first, count)], w_out_all.at[slot, pl.ds(first, count)],
            out_send.at[number], out_recv.at[number],
            device_id=(s, partner), device_id_type=MESH).wait_recv()

    start_phase(0, 0)
    for copy in query_copies():
        copy.start()
    out_copy(*out_sends[8]).start()
    own_out = pltpu.make_async_copy(w_out, w_out_all.at[t], local_sem.at[1])
    own_out.start()

    w_value_t[...] = jnp.transpose(w_value[...].astype(jnp.float32)).astype(jnp.bfloat16)
    top[...] = jnp.full_like(top, masked_score)
    total[...] = jnp.zeros_like(total)
    acc[...] = jnp.zeros_like(acc)

    lanes = lax.broadcasted_iota(jnp.int32, (HALF, 128), 1)

    def set_queries(group, nope_rows, rope_rows):
        wide = rope_rows.astype(jnp.float32)
        turned = pltpu.roll(wide, 64, 1)
        front = lanes < 64
        for head in range(2):
            one = jnp.transpose(nope_rows[:, head * NOPE:(head + 1) * NOPE].astype(jnp.float32))
            low, high = (wide, turned) if head == 0 else (turned, wide)
            for version, tail in enumerate((jnp.where(front, low, 0.0), jnp.where(front, 0.0, high))):
                queries[group, head, version, 0:NOPE, :] = one.astype(jnp.bfloat16)
                queries[group, head, version, NOPE:2 * NOPE, :] = jnp.transpose(tail).astype(jnp.bfloat16)

    hand_on((0,))
    for chunk in range(4):
        out_chunk(chunk)
    set_queries(0, nope[pl.ds(0, HALF), :], turned_queries[pl.ds(0, HALF), :])

    def expand(block):
        for plane in range(2):
            rows = lat[2 * block + plane, pl.ds(0, HALF), :]
            expanded = jnp.dot(rows, w_key[...], preferred_element_type=jnp.float32).astype(jnp.bfloat16)
            tails = tuple(lat[2 * block + plane, pl.ds(HALF, 128), side * 128:(side + 1) * 128] for side in range(2))
            for head in range(2):
                keys[head, pl.ds(plane * HALF, HALF), 0:NOPE] = expanded[:, head * NOPE:(head + 1) * NOPE]
                for quarter in range(4):
                    keys[head, pl.ds(plane * HALF + quarter * 128, 128), NOPE:2 * NOPE] = tails[quarter % 2]
            values_t[:, plane * HALF:(plane + 1) * HALF] = lax.dot_general(
                w_value_t[...], rows, (((1,), (1,)), ((), ())), preferred_element_type=jnp.float32
            ).astype(jnp.bfloat16)

    def fold(group, masked):
        def make(piece_at):
            head, first = piece_at // 2, (piece_at % 2) * 256
            largest = top[group, head, :, first:first + 256]
            for chunk in range(4):
                scores = jnp.dot(
                    keys[head, pl.ds(256 * chunk, 256), :],
                    queries[group, head, chunk % 2, :, first:first + 256],
                    preferred_element_type=jnp.float32)
                if masked:
                    key_at = lax.broadcasted_iota(jnp.int32, scores.shape, 0) + 256 * chunk
                    column = lax.broadcasted_iota(jnp.int32, scores.shape, 1)
                    query_at = column + jnp.where(column >= 128, 128, 0) + (2 * first + 128 * group)
                    scores = jnp.where(key_at <= query_at, scores, masked_score)
                held[piece_at % 2, pl.ds(256 * chunk, 256), :] = scores
                largest = jnp.maximum(largest, jnp.max(scores, axis=0, keepdims=True))
            return largest

        after = make(0)
        for piece_at in range(4):
            following = make(piece_at + 1) if piece_at < 3 else None
            head, first = piece_at // 2, (piece_at % 2) * 256
            columns = slice(first, first + 256)
            before = top[group, head, :, columns]
            offset = after * score_base2
            added = jnp.zeros((1, 256), jnp.float32)
            mixed = jnp.zeros((VDIM, 256), jnp.float32)
            for chunk in range(4):
                weights = jnp.exp2(held[piece_at % 2, pl.ds(256 * chunk, 256), :] * score_base2 - offset)
                added += jnp.sum(weights, axis=0, keepdims=True)
                mixed += jnp.dot(
                    values_t[head * VDIM:(head + 1) * VDIM, 256 * chunk:256 * (chunk + 1)],
                    weights.astype(jnp.bfloat16), preferred_element_type=jnp.float32)
            factor = jnp.exp2((before - after) * score_base2)
            total[group, head, :, columns] = total[group, head, :, columns] * factor + added
            acc[group, head, :, columns] = acc[group, head, :, columns] * factor + mixed
            top[group, head, :, columns] = after
            after = following

    def process(block, place):
        @pl.when(block <= jnp.maximum(s, mirror))
        def _():
            expand(block)

        def one(group, carry):
            last = jnp.where(group == 0, s, mirror)

            @pl.when((place == 0) & (group == 1))
            def _():
                wait_received(0, 0)
                start_phase(0, 1)
                hand_on((1, 2, 3, 4))
                for copy in query_copies():
                    copy.wait_recv()
                set_queries(1, far_nope[...], far_rope[...])

            @pl.when(block < last)
            def _():
                fold(group, False)

            @pl.when(block == last)
            def _():
                fold(group, True)

            return carry

        lax.fori_loop(0, 2, one, 0)

    def advance(place, carry):
        @pl.when(place == 1)
        def _():
            wait_received(0, 1, 0, 4)
            start_phase(0, 2)
            hand_on((5, 6))

        @pl.when(place == 3)
        def _():
            wait_received(0, 1, 4, 12)
            start_phase(0, 3)
            hand_on((7, 8, 9, 10))
            start_phase(1, 0)

        @pl.when(place == 5)
        def _():
            wait_received(0, 2)
            wait_received(0, 3)
            start_phase(0, 4)
            hand_on((11, 12, 13, 14))
            for number in (2, 3, 4, 5):
                out_wait(number)
            for number in (9, 10):
                out_copy(*out_sends[number]).start()

        @pl.when(place == 8)
        def _():
            for number in (0, 1, 6, 7):
                out_wait(number)
            for number in (11, 12):
                out_copy(*out_sends[number]).start()

        @pl.when(place == 10)
        def _():
            wait_received(1, 0)
            start_phase(1, 1, 0, 4)
            start_phase(1, 1, 4, 6)
            start_phase(1, 1, 8, 10)

        @pl.when(place == 13)
        def _():
            start_phase(1, 1, 6, 8)
            start_phase(1, 1, 10, 12)

        @pl.when(place == 11)
        def _():
            wait_received(0, 4)
            hand_on((15,))

        @pl.when((place >= 6) & (place < 15))
        def _():
            side_arrived(place + 1)

        dy = pick(place, [pair[0] for pair in ORDER])
        dz = pick(place, [pair[1] for pair in ORDER])
        block = sp_at(dy, dz)
        theirs = lat.at[2 * block + 1 - core]
        pltpu.make_async_remote_copy(
            theirs, theirs, pair_send.at[place], pair_recv.at[place],
            device_id=(s, partner), device_id_type=MESH).wait_recv()
        process(block, place)
        return carry

    lax.fori_loop(0, 16, advance, 0)

    def head_copy(group, part):
        target = 2 * part + group
        return pltpu.make_async_remote_copy(
            head_out.at[group, pl.ds(128 * part, 128)], heads_all.at[t],
            head_send.at[4 * group + part], head_recv.at[t],
            device_id=(s if group == 0 else mirror, target), device_id_type=MESH)

    def close(group):
        for head in range(2):
            mixed = acc[group, head] / total[group, head]
            head_out[group, :, head * VDIM:(head + 1) * VDIM] = jnp.transpose(mixed).astype(jnp.bfloat16)

    close(1)
    for number in range(4):
        head_copy(1, number).start()
    close(0)
    for number in range(4):
        @pl.when(t != 2 * number)
        def _():
            head_copy(0, number).start()

    @pl.when(core == 0)
    def _():
        mine = pltpu.make_async_copy(
            head_out.at[0, pl.ds(128 * x, 128)], heads_all.at[t], local_sem.at[2])
        mine.start()
        mine.wait()

    def head_wait(slot):
        @pl.when((core == 1) | (slot != t))
        def _():
            pltpu.make_async_remote_copy(
                head_out.at[0, pl.ds(0, 128)], heads_all.at[slot], head_send.at[0], head_recv.at[slot],
                device_id=(mirror, t), device_id_type=MESH).wait_recv()

    wait_received(1, 1, 0, 4)
    start_phase(1, 2)
    for number in (9, 10):
        out_wait(number)
    out_copy(*out_sends[13]).start()
    for number in (8, 11, 12):
        out_wait(number)
    own_out.wait()

    stream[...] = resid[...].astype(jnp.float32)

    def project(turn, carry):
        @pl.when(turn == 7)
        def _():
            out_wait(13)

        slot = pick(turn, (0, 1, 2, 3, 6, 7, 4, 5))
        slot = (2 * x + core + slot - 2 * ((core + slot % 2) // 2)) % 8
        head_wait(slot)
        stream[...] += jnp.dot(heads_all[slot], w_out_all[slot], preferred_element_type=jnp.float32)
        return carry

    lax.fori_loop(0, 8, project, 0)
    rows_f32 = stream[...]
    scale = lax.rsqrt(jnp.mean(rows_f32 * rows_f32, axis=-1, keepdims=True) + norm_eps)
    rows_all[t] = (rows_f32 * scale * mix_gain[...]).astype(jnp.bfloat16)

    high, low = (0, 64), (64, 64)
    all_rows = (0, 128)
    row_sends = (
        (0, t, low, right), (1, t, high, left), (2, t, all_rows, partner),
        (3, right, high, left), (4, left, low, right),
        (5, right, all_rows, partner), (6, left, all_rows, partner), (7, across, all_rows, partner),
        (8, t, high, right), (9, t, low, left),
    )
    row_receives = (
        (0, left, low), (1, right, high), (2, partner, all_rows),
        (3, across, high), (4, across, low),
        (5, other(right), all_rows), (6, other(left), all_rows), (7, other(across), all_rows),
        (8, left, high), (9, right, low),
    )

    def row_copy(number):
        _, slot, (first, count), target = row_sends[number]
        here = rows_all.at[slot, pl.ds(first, count)]
        return pltpu.make_async_remote_copy(
            here, here, row_send.at[number], row_recv.at[number],
            device_id=(s, target), device_id_type=MESH)

    def row_wait(number):
        _, slot, (first, count) = row_receives[number]
        here = rows_all.at[slot, pl.ds(first, count)]
        pltpu.make_async_remote_copy(
            here, here, row_send.at[number], row_recv.at[number],
            device_id=(s, partner), device_id_type=MESH).wait_recv()

    for number in range(3):
        row_copy(number).start()
    wait_received(1, 1, 4, 12)
    start_phase(1, 3)

    def last_weights():
        wait_received(1, 2)
        wait_received(1, 3)
        start_phase(1, 4)

    @pl.when(core == 1)
    def _():
        last_weights()

    row_wait(0)
    row_wait(1)
    for number in (3, 4, 8, 9):
        row_copy(number).start()

    @pl.when(core == 0)
    def _():
        last_weights()

    row_wait(2)
    row_wait(3)
    row_wait(4)
    row_copy(7).start()
    wait_received(1, 4)
    row_wait(7)

    def part_copy(step):
        return pltpu.make_async_remote_copy(
            halves.at[step, 1 - core], got.at[step], part_send.at[step], part_recv.at[step],
            device_id=(s, partner), device_id_type=MESH)

    def chip_total(step):
        part_copy(step).wait_recv()
        return halves[step, core].astype(jnp.float32) + got[step].astype(jnp.float32)

    def sum_copy(number):
        here, there, target = (
            (summed.at[0, pl.ds(0, 64)], relay.at[0], right),
            (summed.at[0, pl.ds(64, 64)], relay.at[1], left),
            (summed.at[1, pl.ds(64, 64)], arrived.at[0, pl.ds(64, 64)], right),
            (summed.at[2, pl.ds(0, 64)], arrived.at[1, pl.ds(0, 64)], left),
            (summed.at[1, pl.ds(0, 64)], arrived.at[0, pl.ds(0, 64)], right),
            (summed.at[2, pl.ds(64, 64)], arrived.at[1, pl.ds(64, 64)], left),
        )[number]
        return pltpu.make_async_remote_copy(
            here, there, sum_send.at[number], sum_recv.at[number],
            device_id=(s, target), device_id_type=MESH)

    def finish(step):
        if step == 3:
            stream[...] += 0.5 * chip_total(3)
        elif step == 0:
            summed[0] = chip_total(0).astype(jnp.bfloat16)
            sum_copy(0).start()
            sum_copy(1).start()
        else:
            total_rows = chip_total(step)
            sent, kept = (slice(64, 128), slice(0, 64)) if step == 1 else (slice(0, 64), slice(64, 128))
            summed[step, sent, :] = total_rows[sent].astype(jnp.bfloat16)
            sum_copy(step + 1).start()
            waiting[step - 1] = total_rows[kept]

    def mix(step, carry):
        @pl.when(step == 1)
        def _():
            row_wait(8)
            row_wait(9)
            row_copy(5).start()
            row_copy(6).start()
            row_wait(5)

        @pl.when(step == 2)
        def _():
            row_wait(6)

        chip = (x + pick(step, (2, 1, 3, 0))) % SIDE

        def columns(pair, first, count):
            return jnp.concatenate([weights_all[2 * pair + side, pl.ds(first, count), :] for side in range(2)], axis=1)

        def product(first, count):
            added = jnp.zeros((256, count), jnp.float32)
            for pair in range(8):
                rows = rows_all[pl.ds(2 * chip, 2), :, 256 * pair:256 * (pair + 1)].reshape(256, 256)
                added += lax.dot_general(
                    rows, columns(pair, first, count), (((1,), (1,)), ((), ())), preferred_element_type=jnp.float32)
            return added

        for first, count in ((0, 256), (256, 256), (512, 192)):
            gate_value, upward = product(first, count), product(UNITS + first, count)
            hidden[:, first:first + count] = (gate_value / (1.0 + jnp.exp(-gate_value)) * upward).astype(jnp.bfloat16)

        for one in range(3):
            @pl.when(step == one + 1)
            def _():
                finish(one)

        for pair in range(8):
            down = jnp.dot(hidden[...], columns(pair, 2 * UNITS, UNITS), preferred_element_type=jnp.float32)
            halves[step, :, :, 256 * pair:256 * (pair + 1)] = down.astype(jnp.bfloat16).reshape(2, 128, 256)
        part_copy(step).start()

        return carry

    lax.fori_loop(0, 4, mix, 0)
    for side in range(2):
        sum_copy(side).wait_recv()
        rows = pl.ds(64 * side, 64)
        summed[1 + side, rows, :] = (waiting[side] + relay[side].astype(jnp.float32)).astype(jnp.bfloat16)
        sum_copy(4 + side).start()
    finish(3)
    sum_copy(2).wait_recv()
    sum_copy(3).wait_recv()
    sum_copy(4).wait_recv()
    sum_copy(5).wait_recv()
    result[...] = (
        stream[...] + 0.5 * (arrived[0].astype(jnp.float32) + arrived[1].astype(jnp.float32))).astype(jnp.bfloat16)

    for number in range(6):
        sum_copy(number).wait_send()
    for step in range(4):
        part_copy(step).wait_send()
    for number in range(10):
        row_copy(number).wait_send()
    for number in range(14):
        out_copy(*out_sends[number]).wait_send()
    for copy in query_copies():
        copy.wait_send()
    for phase in range(len(SENDS)):
        for index in range(len(SENDS[phase])):
            shard_copy(0, phase, index).wait_send()
            shard_copy(1, phase, index).wait_send()
    for place in range(16):
        pair_copy(place).wait_send()
        if place > 6:
            side_copy(place, 0).wait_send()
            side_copy(place, 1).wait_send()
    for number in range(4):
        head_copy(1, number).wait_send()

        @pl.when(t != 2 * number)
        def _():
            head_copy(0, number).wait_send()


def layer_call(*operands):
    vmem = pl.BlockSpec(memory_space=pltpu.VMEM)
    anywhere = pl.BlockSpec(memory_space=pl.ANY)
    dma = pltpu.SemaphoreType.DMA
    bf16, f32 = jnp.bfloat16, jnp.float32
    return pl.pallas_call(
        layer_kernel,
        out_shape=jax.ShapeDtypeStruct((128, 2048), bf16),
        in_specs=[anywhere] * len(operands),
        out_specs=vmem,
        scratch_shapes=[
            pltpu.VMEM((ROWS, 256), bf16),
            pltpu.VMEM((ROWS, 128), bf16),
            pltpu.VMEM((HALF, 256), bf16),
            pltpu.VMEM((ROPE, HALF), bf16),
            pltpu.VMEM((1, 256), f32),
            pltpu.VMEM((256, 256), bf16),
            pltpu.VMEM((256, 256), bf16),
            pltpu.VMEM((128, 2048), bf16),
            pltpu.VMEM((1, 2048), f32),
            pltpu.VMEM((ROWS, 128), f32),
            pltpu.VMEM((ROWS, 128), f32),
            pltpu.VMEM((16, 128), f32),
            pltpu.VMEM((16, 128), f32),
            pltpu.VMEM((ROWS, 128), bf16),
            pltpu.VMEM((32, SHARD, 256), bf16),
            pltpu.VMEM((HALF, 256), bf16),
            pltpu.VMEM((HALF, 128), bf16),
            pltpu.VMEM((2, 2, 2, 256, HALF), bf16),
            pltpu.VMEM((2, ROWS, 256), bf16),
            pltpu.VMEM((256, ROWS), bf16),
            pltpu.VMEM((2, ROWS, 256), f32),
            pltpu.VMEM((256, 256), bf16),
            pltpu.VMEM((2, 2, 1, HALF), f32),
            pltpu.VMEM((2, 2, 1, HALF), f32),
            pltpu.VMEM((2, 2, VDIM, HALF), f32),
            pltpu.VMEM((2, HALF, 256), bf16),
            pltpu.VMEM((8, 128, 256), bf16),
            pltpu.VMEM((8, 256, 2048), bf16),
            pltpu.VMEM((16, 3 * UNITS, 128), bf16),
            pltpu.VMEM((256, UNITS), bf16),
            pltpu.VMEM((128, 2048), f32),
            pltpu.VMEM((8, 128, 2048), bf16),
            pltpu.VMEM((4, 2, 128, 2048), bf16),
            pltpu.VMEM((4, 128, 2048), bf16),
            pltpu.VMEM((3, 128, 2048), bf16),
            pltpu.VMEM((2, 64, 2048), bf16),
            pltpu.VMEM((2, 128, 2048), bf16),
            pltpu.VMEM((2, 64, 2048), f32),
            dma((32,)), dma((64,)), dma((18,)), dma((18,)), dma((16,)), dma((16,)), dma((2,)), dma((2,)),
            dma((8,)), dma((8,)), dma((14,)), dma((14,)), dma((4,)),
            dma((32,)), dma((64,)), dma((10,)), dma((10,)), dma((4,)), dma((4,)), dma((6,)), dma((6,)), dma((30,)),
        ],
        compiler_params=pltpu.CompilerParams(
            collective_id=0, has_side_effects=True, vmem_limit_bytes=67_000_000),
        cost_estimate=pl.CostEstimate(flops=60_000_000_000, bytes_accessed=30_000_000, transcendentals=18_000_000),
        name="layer",
    )(*operands)


def angle_tables(positions):
    frequency = theta_base ** (-2.0 * np.arange(ROPE // 2) / ROPE)
    angle = np.tile(np.asarray(positions, np.float64)[:, None] * frequency[None, :], (1, 4))
    return np.cos(angle).astype(np.float32), np.sin(angle).astype(np.float32)


def on_device(
    resid, query_nope, query_rope, latent, key_rope, latent_gain, w_key, w_value, w_out, mix_gain,
    w_gate, w_up, w_down,
):
    row_tables = angle_tables(np.arange(ROWS))
    block_tables = angle_tables(ROWS * np.arange(16))
    return layer_call(
        query_nope, query_rope, latent, key_rope.T, latent_gain.reshape(1, -1), w_key, w_value, w_out, resid,
        mix_gain.reshape(1, -1), w_gate.T, w_up.T, w_down.T,
        *(jnp.asarray(table) for table in row_tables + block_tables))


def solution(mesh):
    return jax.shard_map(
        on_device,
        mesh=mesh,
        in_specs=(
            P(("sp", "tp"), None),
            P("sp", "tp"),
            P("sp", "tp"),
            P("sp", None),
            P("sp", None),
            P(),
            P(None, "tp"),
            P(None, "tp"),
            P("tp", None),
            P(),
            P("sp", "tp"),
            P("sp", "tp"),
            P("sp", "tp"),
        ),
        out_specs=P(("sp", "tp"), None),
        check_vma=False,
    )
```
